32 devices in a mesh: ep: 8 (over z, x), tp: 4 (over y, core).
Axes of the slice: x: 2, y: 2, z: 4, core: 2. Of those that a mesh axis runs over, the one named last changes fastest.
Arguments:
- conv_value: bfloat16 [1024, 4096], P('tp', 'ep'), may hold values from -6 to 6
- conv_gate: bfloat16 [1024, 4096], P('tp', 'ep'), may hold values from -8 to 8
- conv_kernel: bfloat16 [31, 1024], P(None, 'tp'), may hold values from -1 to 1
- norm_gain: float32 [1024], replicated, may hold values from 0.1 to 1.9
- norm_shift: float32 [1024], replicated, may hold values from -3 to 3
- out_weight: bfloat16 [1024, 4096], P(None, 'tp'), may hold values from -0.1875 to 0.1875
- expert_input: bfloat16 [1024, 4096], P('ep'), may hold values from -6 to 6
- expert_ids: int32 [1024, 2], P('ep'), may hold values from 0 to 7, as said below
- pair_logits: float32 [1024, 2], P('ep'), may hold values from -6 to 6
- group_prob: float32 [1024], P('ep'), may hold values from 0.3 to 1
- expert_gate: bfloat16 [8, 4096, 2048], P('ep', None, 'tp'), may hold values from -0.09375 to 0.09375
- expert_up: bfloat16 [8, 4096, 2048], P('ep', None, 'tp'), may hold values from -0.09375 to 0.09375
- expert_down: bfloat16 [8, 2048, 4096], P('ep', None, 'tp'), may hold values from -0.125 to 0.125
Outputs:
- mixer_out: bfloat16 [4096, 4096], P('ep', 'tp')
- expert_out: bfloat16 [1024, 4096], P('ep', 'tp')
The draws below stay inside these ranges and needn't reach their ends.
Inputs may be any that keep to these rules, and one draw needn't show every extreme that they name: `expert_ids`: the two experts of a token differ and lie in one group, ids g * 2 to (g + 1) * 2 - 1 for some g. The 128 tokens of one index of ep name every expert exactly 32 times.
All inputs are finite; a program needn't handle non-finite values.
Results may differ from the reference program's by a relative error of at most 0.0064.
Values may be sent and summed in bfloat16 or wider, within the bound.
A program may use at most 64 MiB of HBM per device.

```python
import jax
import jax.numpy as jnp
from jax import lax

D = 4096
CONV_CH = 1024
KERNEL = 31
EXPERT_FF = 2048
GROUPS = 4
B_DEV = 128
EXPERTS = 8
TOK_A = 4096
TOK_B = 1024


def draw_expert_ids(key, part):
    group_size = EXPERTS // GROUPS
    blocks = TOK_B // B_DEV

    def one_block(block_key):
        key_order, key_offset, key_stride = jax.random.split(block_key, 3)
        order = jax.random.permutation(key_order, B_DEV)
        places = jnp.arange(B_DEV, dtype=jnp.int32)
        group = places % GROUPS
        ordinal = places // GROUPS
        offsets = jax.random.randint(key_offset, (GROUPS,), 0, group_size)
        strides = jax.random.randint(key_stride, (GROUPS,), 0, group_size - 1)
        first = (ordinal + offsets[group]) % group_size
        second = (first + 1 + strides[group]) % group_size
        chosen = jnp.stack([group * group_size + first, group * group_size + second], axis=1).astype(jnp.int32)
        return jnp.zeros((B_DEV, 2), jnp.int32).at[order].set(chosen)
    block_keys = jax.random.split(jax.random.fold_in(key, 17), blocks)
    return jax.vmap(one_block)(block_keys).reshape(TOK_B, 2).astype(jnp.int32)


def block_levels(stream_key, dims, shards, low, largest):
    level, own = 1.0, jax.random.fold_in(stream_key, 6)
    for dim, shards_of in shards:
        steps = jnp.exp(jax.random.uniform(jax.random.fold_in(own, dim), (shards_of,), jnp.float32, low / len(shards), largest / len(shards)))
        level = level * jnp.repeat(steps, dims[dim] // shards_of).reshape([-1 if axis == dim else 1 for axis in range(len(dims))])
    return level


def gaussian(stream_key, dims, scale, bound, cuts=(), held_as=jnp.bfloat16):
    factor_of = block_levels(stream_key, dims, cuts, -0.22, 0.18) if cuts else 1.0
    drawn = jax.random.normal(stream_key, dims, jnp.float32) * scale * factor_of
    return jnp.minimum(jnp.maximum(drawn, -bound), bound).astype(held_as)


def setup_inputs(seed: int = 0) -> dict:
    key_of = jax.random.split(jax.random.key(seed), 14)
    return {
        "conv_value": gaussian(key_of[0], (CONV_CH, TOK_A), 1.0, 6.0, ((0, 4), (1, 8))),
        "conv_gate": gaussian(key_of[1], (CONV_CH, TOK_A), 1.5, 8.0, ((0, 4), (1, 8))),
        "conv_kernel": gaussian(key_of[2], (KERNEL, CONV_CH), KERNEL ** -0.5, 1.0, ((1, 4),)),
        "norm_gain": jnp.clip(1.0 + 0.18 * jax.random.normal(key_of[3], (CONV_CH,), jnp.float32), 0.1, 1.9),
        "norm_shift": gaussian(key_of[4], (CONV_CH,), 0.5, 3.0, (), jnp.float32),
        "out_weight": gaussian(key_of[5], (CONV_CH, D), CONV_CH ** -0.5, 0.1875, ((1, 4),)),
        "expert_input": gaussian(key_of[6], (TOK_B, D), 1.0, 6.0, ((0, 8),)),
        "expert_ids": draw_expert_ids(jax.random.fold_in(key_of[13], 71), 0),
        "pair_logits": gaussian(key_of[8], (TOK_B, 2), 1.5, 6.0, ((0, 8),), jnp.float32),
        "group_prob": jnp.clip(0.3 + 0.7 * jax.random.uniform(key_of[9], (TOK_B,), jnp.float32) ** block_levels(key_of[9], (TOK_B,), ((0, 8),), -0.2, 0.2), 0.3, 1.0),
        "expert_gate": gaussian(key_of[10], (EXPERTS, D, EXPERT_FF), D ** -0.5, 0.09375, ((0, 8), (2, 4))),
        "expert_up": gaussian(key_of[11], (EXPERTS, D, EXPERT_FF), D ** -0.5, 0.09375, ((0, 8), (2, 4))),
        "expert_down": gaussian(key_of[12], (EXPERTS, EXPERT_FF, D), EXPERT_FF ** -0.5, 0.125, ((0, 8), (2, 4))),
    }


def norm_swish(conv_out, norm_gain, norm_shift):
    values = conv_out.astype(jnp.float32)
    center = lax.optimization_barrier(jnp.mean(values, axis=0, keepdims=True))
    spread = lax.optimization_barrier(jnp.mean(jnp.square(values - center), axis=0, keepdims=True))
    normed = (values - center) * lax.rsqrt(spread + 1e-05) * norm_gain[:, None] + norm_shift[:, None]
    return jax.nn.silu(normed).astype(jnp.bfloat16)

def route_weights(pair_logits, group_prob):
    share = jax.nn.sigmoid(pair_logits[:, 0] - pair_logits[:, 1])
    return jnp.stack([share, 1.0 - share], axis=1) * group_prob[:, None]

def reference(conv_value, conv_gate, conv_kernel, norm_gain, norm_shift, out_weight, expert_input, expert_ids, pair_logits, group_prob, expert_gate, expert_up, expert_down):
    gated = (conv_value.astype(jnp.float32) * jax.nn.sigmoid(conv_gate.astype(jnp.float32))).astype(jnp.bfloat16)
    reach = (KERNEL - 1) // 2
    length = gated.shape[1]
    padded = jnp.pad(gated.astype(jnp.float32), ((0, 0), (reach, reach)))
    kernel_f = conv_kernel.astype(jnp.float32)
    summed = jnp.zeros(gated.shape, jnp.float32)
    for offset in range(KERNEL):
        summed = summed + kernel_f[offset][:, None] * padded[:, offset:offset + length]
    conv_out = summed.astype(jnp.bfloat16)
    swished = norm_swish(conv_out, norm_gain, norm_shift)
    mixer_out = lax.dot_general(swished, out_weight, (((0,), (0,)), ((), ())), preferred_element_type=jnp.float32).astype(jnp.bfloat16)
    weights = route_weights(pair_logits, group_prob)
    flat = expert_ids.reshape(-1).astype(jnp.int32)
    order = jnp.argsort(flat, stable=True).astype(jnp.int32)
    experts_all = expert_gate.shape[0]
    per_expert = flat.shape[0] // experts_all
    rows = (order // 2).astype(jnp.int32).reshape(experts_all, per_expert)

    def one_expert(packed):
        rows_here, gate_w, up_w, down_w = packed
        block = expert_input[rows_here]
        gate_val = jnp.dot(block, gate_w, preferred_element_type=jnp.float32)
        up_val = jnp.dot(block, up_w, preferred_element_type=jnp.float32)
        hidden = (jax.nn.silu(gate_val) * up_val).astype(jnp.bfloat16)
        return jnp.dot(hidden, down_w, preferred_element_type=jnp.float32).astype(jnp.bfloat16)
    results = lax.map(one_expert, (rows, expert_gate, expert_up, expert_down))
    width = expert_input.shape[1]
    copies = jnp.zeros((flat.shape[0], width), jnp.bfloat16).at[order].set(results.reshape(-1, width))
    copies = copies.reshape(-1, 2, width).astype(jnp.float32)
    expert_out = lax.optimization_barrier(jnp.sum(copies * weights[:, :, None], axis=1)).astype(jnp.bfloat16)
    return (mixer_out, expert_out)
```

```python
import functools

import jax
import jax.numpy as jnp
from jax import lax
from jax.experimental import pallas as pl
from jax.experimental.pallas import tpu as pltpu
from jax.sharding import PartitionSpec as P

MESH = pl.DeviceIdType.MESH
CORES = 2
PAIR = 2
GROUPS = 4
F32, BF16 = jnp.float32, jnp.bfloat16


def tiles(size, most):
    tile = min(size, most)
    return tile, size // tile


def kernel(
    experts,
    parts,
    value_hbm,
    gate_hbm,
    input_hbm,
    wgate_hbm,
    wup_hbm,
    wdown_hbm,
    wout_hbm,
    taps_ref,
    gain_ref,
    shift_ref,
    ids_ref,
    logits_ref,
    prob_ref,
    mixer_hbm,
    expert_hbm,
    value,
    gate,
    tokens,
    wgate,
    wup,
    wdown,
    wout,
    send_rows,
    arrived,
    gate_sum,
    up_sum,
    hidden,
    down_sum,
    result,
    returned,
    padded,
    edges,
    halo,
    conv,
    swished,
    mixer,
    combined,
    load_sem,
    out_sem,
    self_sem,
    disp_send,
    disp_recv,
    fwd_send,
    fwd_recv,
    hal_send,
    hal_recv,
    conv_send,
    conv_recv,
    hid_send,
    hid_recv,
    ret_send,
    ret_recv,
):
    me = lax.axis_index("ep")
    tp = lax.axis_index("tp")
    chips = parts // CORES
    chip, core = lax.div(tp, CORES), lax.rem(tp, CORES)
    other = 1 - core
    sibling = chip * CORES + other
    slots = send_rows.shape[1]
    half = send_rows.shape[2]
    rows = experts * slots
    length, channels = conv.shape[1], conv.shape[2]
    edge = halo.shape[1]
    reach = (taps_ref.shape[0] - 1) // 2

    def remote(src, dst, ssem, rsem, ep=None, part=None):
        target = (me if ep is None else ep, tp if part is None else part)
        return pltpu.make_async_remote_copy(
            src_ref=src, dst_ref=dst, send_sem=ssem, recv_sem=rsem, device_id=target, device_id_type=MESH
        )

    def ahead(k):
        return lax.rem(me + k, experts)

    def behind(k):
        return lax.rem(me + experts - k, experts)

    def chip_ahead(k):
        return lax.rem(chip + k, chips) * CORES + core

    def chip_behind(k):
        return lax.rem(chip + chips - k, chips) * CORES + core

    barrier = pltpu.get_barrier_semaphore()

    @pl.loop(1, experts)
    def _(k):
        pl.semaphore_signal(barrier, inc=1, device_id=(ahead(k), tp), device_id_type=MESH)

    @pl.loop(1, chips)
    def _(k):
        pl.semaphore_signal(barrier, inc=1, device_id=(me, chip_ahead(k)), device_id_type=MESH)

    pl.semaphore_signal(barrier, inc=1, device_id=(me, sibling), device_id_type=MESH)

    columns = pl.ds(pl.multiple_of(core * half, half), half)
    loads = [
        pltpu.make_async_copy(src, dst, load_sem.at[i])
        for i, (src, dst) in enumerate(
            [
                (input_hbm.at[:, columns], tokens),
                (value_hbm, value),
                (gate_hbm, gate),
                (wgate_hbm.at[0], wgate),
                (wup_hbm.at[0], wup),
                (wout_hbm, wout),
                (wdown_hbm.at[0], wdown),
            ]
        )
    ]
    for load in loads:
        load.start()

    count = ids_ref.shape[1]
    first, second = ids_ref[0:1, :], ids_ref[1:2, :]
    expert_of = lax.broadcasted_iota(jnp.int32, (experts, count), 0)
    is_first, is_second = expert_of == first, expert_of == second
    chosen = jnp.where(is_first | is_second, 1.0, 0.0).astype(F32)
    earlier = lax.broadcasted_iota(jnp.int32, (count, count), 0) < lax.broadcasted_iota(
        jnp.int32, (count, count), 1
    )
    rank = jnp.dot(
        chosen.astype(BF16), jnp.where(earlier, 1.0, 0.0).astype(BF16), preferred_element_type=F32
    )
    rank = jnp.where(chosen > 0, rank, -1.0)
    ordinal = lax.broadcasted_iota(jnp.int32, (experts, slots, count), 1).astype(F32)
    place3 = jnp.broadcast_to(rank[:, None, :], (experts, slots, count)) == ordinal
    place = jnp.where(place3, 1.0, 0.0).astype(F32).reshape(rows, count)

    loads[0].wait()
    tile, steps = tiles(half, 512)
    for i in range(steps):
        span = slice(i * tile, (i + 1) * tile)
        picked = jnp.dot(place.astype(BF16), tokens[:, span], preferred_element_type=F32)
        send_rows[:, :, span] = picked.reshape(experts, slots, tile).astype(BF16)

    pl.semaphore_wait(barrier, experts - 1 + chips)

    def dispatch(k):
        return remote(
            send_rows.at[ahead(k)], arrived.at[core, me], disp_send.at[k], disp_recv.at[k], ep=ahead(k)
        )

    def forward(k, src):
        return remote(
            src, arrived.at[core, behind(k)], fwd_send.at[k], fwd_recv.at[k], part=sibling
        )

    @pl.loop(1, experts)
    def _(k):
        dispatch(k).start()

    keep = pltpu.make_async_copy(send_rows.at[me], arrived.at[core, me], self_sem.at[0])
    keep.start()
    forward(0, send_rows.at[me]).start()

    loads[1].wait()
    loads[2].wait()
    gated = (value[...].astype(F32) * jax.nn.sigmoid(gate[...].astype(F32))).astype(BF16)
    padded[edge : edge + length, :] = jnp.transpose(gated.astype(F32), (1, 0))
    edges[0] = padded[edge : 2 * edge, :].astype(BF16)
    edges[1] = padded[length : length + edge, :].astype(BF16)
    to_left = remote(edges.at[0], halo.at[1], hal_send.at[0], hal_recv.at[0], ep=behind(1))
    to_right = remote(edges.at[1], halo.at[0], hal_send.at[1], hal_recv.at[1], ep=ahead(1))
    to_left.start()
    to_right.start()
    taps = taps_ref[...].astype(F32)
    chunk, chunks = tiles(length, 64)

    def convolve(i):
        total = jnp.zeros((chunk, channels), F32)
        for j in range(taps.shape[0]):
            start = i * chunk + j + edge - reach
            total = total + taps[j : j + 1, :] * padded[start : start + chunk, :]
        conv[tp, i * chunk : (i + 1) * chunk, :] = total.astype(BF16)

    for i in range(1, chunks - 1):
        convolve(i)
    to_left.wait()
    to_right.wait()
    padded[0:edge, :] = jnp.where(me == 0, 0.0, halo[0].astype(F32))
    padded[edge + length : 2 * edge + length, :] = jnp.where(
        me == experts - 1, 0.0, halo[1].astype(F32)
    )
    convolve(0)
    convolve(chunks - 1)

    def gather(buffer, ssem, rsem):
        def across(k):
            return remote(buffer.at[tp], buffer.at[tp], ssem.at[k], rsem.at[k], part=chip_ahead(k))

        def beside(k):
            block = chip_behind(k)
            return remote(
                buffer.at[block], buffer.at[block], ssem.at[chips + k], rsem.at[chips + k], part=sibling
            )

        return across, beside

    conv_across, conv_beside = gather(conv, conv_send, conv_recv)

    @pl.loop(1, chips)
    def _(k):
        conv_across(k).start()

    conv_beside(0).start()

    @pl.loop(1, experts)
    def _(k):
        dispatch(k).wait_recv()
        forward(k, arrived.at[core, behind(k)]).start()

    keep.wait()
    loads[3].wait()
    loads[4].wait()
    units = gate_sum.shape[1]
    tile, steps = tiles(units, 256)

    def side(which):
        block = arrived[which]
        if slots % 16:
            return block.astype(F32).reshape(rows, half).astype(BF16)
        return block.reshape(rows, half)

    def depth(which):
        return pl.ds(pl.multiple_of(which * half, half), half)

    for i in range(steps):
        span = slice(i * tile, (i + 1) * tile)
        gate_sum[:, span] = jnp.dot(side(core), wgate[depth(core), span], preferred_element_type=F32)
        up_sum[:, span] = jnp.dot(side(core), wup[depth(core), span], preferred_element_type=F32)

    @pl.loop(0, experts)
    def _(k):
        forward(k, send_rows.at[me]).wait_recv()

    for i in range(steps):
        span = slice(i * tile, (i + 1) * tile)
        gate_val = gate_sum[:, span] + jnp.dot(
            side(other), wgate[depth(other), span], preferred_element_type=F32
        )
        up_val = up_sum[:, span] + jnp.dot(
            side(other), wup[depth(other), span], preferred_element_type=F32
        )
        hidden[tp, :, span] = (jax.nn.silu(gate_val) * up_val).astype(BF16)

    hid_across, hid_beside = gather(hidden, hid_send, hid_recv)

    @pl.loop(1, chips)
    def _(k):
        hid_across(k).start()

    hid_beside(0).start()

    @pl.loop(1, chips)
    def _(k):
        conv_across(k).wait_recv()
        conv_beside(k).start()

    @pl.loop(0, chips)
    def _(k):
        conv_beside(k).wait_recv()

    width = parts * channels
    chunk, chunks = tiles(length, 64)

    @pl.loop(0, chunks)
    def _(i):
        span = pl.ds(pl.multiple_of(i * chunk, chunk), chunk)
        blocks = [conv[b, span, :].astype(F32) for b in range(parts)]
        center = sum(jnp.sum(block, axis=1, keepdims=True) for block in blocks) / width
        blocks = [block - center for block in blocks]
        spread = sum(jnp.sum(block * block, axis=1, keepdims=True) for block in blocks) / width
        scale = lax.rsqrt(spread + 1e-05)
        for b in range(parts):
            lanes = slice(b * channels, (b + 1) * channels)
            normed = blocks[b] * scale * gain_ref[:, lanes] + shift_ref[:, lanes]
            swished[b, span, :] = jax.nn.silu(normed).astype(BF16)

    loads[6].wait()
    wide = down_sum.shape[1]
    tile, steps = tiles(wide, 256)

    def down(block, begin):
        deep = pl.ds(pl.multiple_of(block * units, units), units)

        @pl.loop(0, steps)
        def _(i):
            span = pl.ds(pl.multiple_of(i * tile, tile), tile)
            product = jnp.dot(hidden[block], wdown[deep, span], preferred_element_type=F32)
            down_sum[:, span] = product if begin else down_sum[:, span] + product

    down(tp, True)
    hid_beside(0).wait_recv()
    down(sibling, False)

    @pl.loop(1, chips)
    def _(k):
        hid_across(k).wait_recv()
        hid_beside(k).start()
        down(chip_behind(k), False)
        hid_beside(k).wait_recv()
        down(chip_behind(k) + other - core, False)

    result[...] = down_sum[...].reshape(experts, slots, wide).astype(BF16)

    def give_back(k):
        return remote(result.at[ahead(k)], returned.at[me], ret_send.at[k], ret_recv.at[k], ep=ahead(k))

    @pl.loop(1, experts)
    def _(k):
        give_back(k).start()

    own = pltpu.make_async_copy(result.at[me], returned.at[me], self_sem.at[1])
    own.start()

    loads[5].wait()
    tile, steps = tiles(mixer.shape[1], 256)

    @pl.loop(0, steps)
    def _(i):
        span = pl.ds(pl.multiple_of(i * tile, tile), tile)
        total = jnp.zeros((length, tile), F32)
        for b in range(parts):
            total = total + jnp.dot(
                swished[b], wout[b * channels : (b + 1) * channels, span], preferred_element_type=F32
            )
        mixer[:, span] = total.astype(BF16)

    put_mixer = pltpu.make_async_copy(mixer, mixer_hbm, out_sem.at[0])
    put_mixer.start()

    share = jax.nn.sigmoid(logits_ref[0:1, :] - logits_ref[1:2, :])
    weight = jnp.where(is_first, share * prob_ref[...], 0.0) + jnp.where(
        is_second, (1.0 - share) * prob_ref[...], 0.0
    )
    weights = jnp.where(
        place3, jnp.broadcast_to(weight[:, None, :], (experts, slots, count)), 0.0
    ).reshape(rows, count)
    weights = jnp.transpose(weights, (1, 0))
    high = weights.astype(BF16)
    rest = weights - high.astype(F32)
    middle = rest.astype(BF16)
    low = (rest - middle.astype(F32)).astype(BF16)

    own.wait()

    @pl.loop(1, experts)
    def _(k):
        give_back(k).wait_recv()

    tile, steps = tiles(wide, 512)
    for i in range(steps):
        span = slice(i * tile, (i + 1) * tile)
        block = returned[:, :, span]
        if slots % 16:
            block = block.astype(F32).reshape(rows, tile).astype(BF16)
        else:
            block = block.reshape(rows, tile)
        total = jnp.dot(low, block, preferred_element_type=F32)
        total = total + jnp.dot(middle, block, preferred_element_type=F32)
        total = total + jnp.dot(high, block, preferred_element_type=F32)
        combined[:, span] = total.astype(BF16)

    put_expert = pltpu.make_async_copy(combined, expert_hbm, out_sem.at[1])
    put_expert.start()

    @pl.loop(1, experts)
    def _(k):
        dispatch(k).wait_send()
        give_back(k).wait_send()

    @pl.loop(0, experts)
    def _(k):
        forward(k, send_rows.at[me]).wait_send()

    @pl.loop(1, chips)
    def _(k):
        conv_across(k).wait_send()
        hid_across(k).wait_send()

    @pl.loop(0, chips)
    def _(k):
        conv_beside(k).wait_send()
        hid_beside(k).wait_send()

    put_mixer.wait()
    put_expert.wait()


def pair_kernel(
    groups,
    parts,
    value_hbm,
    gate_hbm,
    input_hbm,
    wgate_hbm,
    wup_hbm,
    wdown_hbm,
    wout_hbm,
    taps_ref,
    gain_ref,
    shift_ref,
    ids_ref,
    logits_ref,
    prob_ref,
    mixer,
    combined,
    value,
    gate,
    mine,
    tokens,
    wgate,
    wup,
    wdown,
    wout,
    send_rows,
    weights,
    arrived_weights,
    arrived,
    gate_sum,
    up_sum,
    hidden,
    down_sum,
    result,
    other_result,
    summed,
    returned,
    scatter,
    padded,
    edges,
    halo,
    conv,
    swished,
    load_sem,
    z_send,
    z_recv,
    w_send,
    w_recv,
    y_send,
    y_recv,
    x_send,
    x_recv,
    d_send,
    d_recv,
    s_send,
    s_recv,
    hal_send,
    hal_recv,
    conv_send,
    conv_recv,
    hid_send,
    hid_recv,
    res_send,
    res_recv,
    ret_send,
    ret_recv,
):
    experts = groups * PAIR
    me = lax.axis_index("ep")
    tp = lax.axis_index("tp")
    group, side = lax.div(me, PAIR), lax.rem(me, PAIR)
    mate = group * PAIR + 1 - side
    chip, core = lax.div(tp, CORES), lax.rem(tp, CORES)
    sibling = chip * CORES + 1 - core
    beside = (1 - chip) * CORES + core
    opposite = (1 - chip) * CORES + 1 - core
    slots, quarter = send_rows.shape[1], send_rows.shape[2]
    order = list(range(0, groups, 2)) + list(range(1, groups, 2))
    spans = 2
    per = groups // spans
    rows = per * PAIR * slots
    length, channels = conv.shape[1], conv.shape[2]
    edge = halo.shape[1]
    reach = (taps_ref.shape[0] - 1) // 2

    def remote(src, dst, ssem, rsem, ep=None, part=None):
        target = (me if ep is None else ep, tp if part is None else part)
        return pltpu.make_async_remote_copy(
            src_ref=src, dst_ref=dst, send_sem=ssem, recv_sem=rsem, device_id=target, device_id_type=MESH
        )

    def onward(k):
        return lax.rem(group + k, groups) * PAIR + side

    def backward(k):
        return lax.rem(group + groups - k, groups) * PAIR + side

    left, right = lax.rem(me + experts - 1, experts), lax.rem(me + 1, experts)
    barrier = pltpu.get_barrier_semaphore()
    peers = [(onward(k), tp) for k in range(1, groups)]
    peers += [(mate, tp), (me, beside), (me, sibling), (left, tp), (right, tp)]
    for peer in peers:
        pl.semaphore_signal(barrier, inc=1, device_id=peer, device_id_type=MESH)

    columns = pl.ds(pl.multiple_of(tp * quarter, quarter), quarter)
    loads = [
        pltpu.make_async_copy(src, dst, load_sem.at[i])
        for i, (src, dst) in enumerate(
            [
                (input_hbm.at[:, columns], mine),
                (input_hbm, tokens),
                (value_hbm, value),
                (gate_hbm, gate),
                (wgate_hbm.at[0], wgate),
                (wup_hbm.at[0], wup),
                (wdown_hbm.at[0], wdown),
                (wout_hbm, wout),
            ]
        )
    ]
    for load in loads:
        load.start()

    count = ids_ref.shape[1]
    first, second = ids_ref[0:1, :], ids_ref[1:2, :]
    position = lax.broadcasted_iota(jnp.int32, (groups, count), 0) + group
    position = jnp.where(position >= groups, position - groups, position) * PAIR
    chosen = jnp.where((first >= position) & (first < position + PAIR), 1.0, 0.0).astype(F32)
    earlier = lax.broadcasted_iota(jnp.int32, (count, count), 0) < lax.broadcasted_iota(
        jnp.int32, (count, count), 1
    )
    rank = jnp.dot(
        chosen.astype(BF16), jnp.where(earlier, 1.0, 0.0).astype(BF16), preferred_element_type=F32
    )
    rank = jnp.where(chosen > 0, rank, -1.0)
    ordinal = lax.broadcasted_iota(jnp.int32, (groups, slots, count), 1).astype(F32)
    place3 = jnp.broadcast_to(rank[:, None, :], (groups, slots, count)) == ordinal
    place_f = jnp.where(place3, 1.0, 0.0).astype(F32).reshape(groups * slots, count)
    place = place_f.astype(BF16)

    def dispatch(k):
        return remote(
            send_rows.at[k - 1],
            arrived.at[tp, order.index(k), 0],
            z_send.at[k],
            z_recv.at[k],
            ep=onward(k),
        )

    loads[0].wait()
    picked = jnp.dot(place[slots:], mine[...], preferred_element_type=F32)
    send_rows[...] = picked.astype(BF16).reshape(groups - 1, slots, quarter)
    pl.semaphore_wait(barrier, len(peers))
    for k in order[1:]:
        dispatch(k).start()

    def to_beside(p):
        return remote(
            arrived.at[tp, p, 0], arrived.at[tp, p, 0], y_send.at[p], y_recv.at[p], part=beside
        )

    def to_mate(p):
        return remote(arrived.at[tp, p, 0], arrived.at[tp, p, 1], x_send.at[p], x_recv.at[p], ep=mate)

    def across(p):
        if p == 0:
            return remote(
                arrived.at[beside, 0, 0], arrived.at[beside, 0, 1], d_send.at[0], d_recv.at[0], ep=mate
            )
        lead = core == 0
        block = jnp.where(lead, tp, beside)
        return remote(
            arrived.at[block, p, 1 - core],
            arrived.at[block, p, 1],
            d_send.at[p],
            d_recv.at[p],
            ep=jnp.where(lead, me, mate),
            part=jnp.where(lead, beside, tp),
        )

    def to_sibling(p, far, which):
        block = beside if far else tp
        i = 4 * p + 2 * which + far
        return remote(
            arrived.at[block, p, which], arrived.at[block, p, which], s_send.at[i], s_recv.at[i], part=sibling
        )

    loads[1].wait()
    for q in range(parts):
        picked = jnp.dot(
            place[:slots], tokens[:, q * quarter : (q + 1) * quarter], preferred_element_type=F32
        )
        arrived[q, 0, 0] = picked.astype(BF16)
    to_mate(0).start()
    across(0).start()

    share = jax.nn.sigmoid(logits_ref[0:1, :] - logits_ref[1:2, :])
    of_first = share * prob_ref[...]
    of_second = (1.0 - share) * prob_ref[...]
    first_mine = (first < second) == (side == 0)
    own_weight = jnp.sum(place_f * jnp.where(first_mine, of_first, of_second), axis=1, keepdims=True)
    mate_weight = jnp.sum(place_f * jnp.where(first_mine, of_second, of_first), axis=1, keepdims=True)
    lane = lax.broadcasted_iota(jnp.int32, (groups * slots, weights.shape[2]), 1)
    both = jnp.where(lane < weights.shape[2] // 2, own_weight, mate_weight)
    weights[...] = both.reshape(weights.shape)

    def give_weights(k):
        return remote(weights.at[k], arrived_weights.at[k], w_send.at[k], w_recv.at[k], ep=onward(k))

    for k in order[1:]:
        give_weights(k).start()
    arrived_weights[0] = weights[0]
    scatter[...] = jnp.transpose(place_f, (1, 0)).astype(BF16)

    loads[2].wait()
    loads[3].wait()
    gated = (value[...].astype(F32) * jax.nn.sigmoid(gate[...].astype(F32))).astype(BF16)
    padded[edge : edge + length, :] = jnp.transpose(gated.astype(F32), (1, 0))
    edges[0] = padded[edge : 2 * edge, :].astype(BF16)
    edges[1] = padded[length : length + edge, :].astype(BF16)
    to_left = remote(edges.at[0], halo.at[1], hal_send.at[0], hal_recv.at[0], ep=left)
    to_right = remote(edges.at[1], halo.at[0], hal_send.at[1], hal_recv.at[1], ep=right)
    to_left.start()
    to_right.start()
    taps = taps_ref[...].astype(F32)
    chunk, chunks = tiles(length, 64)

    def convolve(i):
        total = jnp.zeros((chunk, channels), F32)
        for j in range(taps.shape[0]):
            start = i * chunk + j + edge - reach
            total = total + taps[j : j + 1, :] * padded[start : start + chunk, :]
        conv[tp, i * chunk : (i + 1) * chunk, :] = total.astype(BF16)

    def landed(p):
        dispatch(order[p]).wait_recv()
        to_beside(p).start()
        to_mate(p).start()
        to_sibling(p, 0, 0).start()

    def turned(p):
        if p:
            to_beside(p).wait_recv()
        to_mate(p).wait_recv()
        if p:
            across(p).start()
            to_sibling(p, 1, 0).start()
        to_sibling(p, 0, 1).start()

    def closed(p):
        across(p).wait_recv()
        to_sibling(p, 1, 1).start()

    inner = list(range(1, chunks - 1))
    early = inner[: len(inner) // 3]
    middle = inner[len(inner) // 3 : 2 * len(inner) // 3]
    late = inner[2 * len(inner) // 3 :]
    for i in early:
        convolve(i)
    landed(1)
    turned(0)
    for i in middle:
        convolve(i)
    closed(0)
    for p in range(2, groups):
        landed(p)
    for i in late:
        convolve(i)
    turned(1)
    to_left.wait()
    to_right.wait()
    padded[0:edge, :] = jnp.where(me == 0, 0.0, halo[0].astype(F32))
    padded[edge + length : 2 * edge + length, :] = jnp.where(
        me == experts - 1, 0.0, halo[1].astype(F32)
    )
    convolve(0)
    turned(2)
    convolve(chunks - 1)
    for p in range(3, groups):
        turned(p)

    cuts = 2
    share_rows = length // cuts

    def conv_copy(i, kind):
        cut = pl.ds(i * share_rows, share_rows)
        block = beside if kind == 2 else tp
        j = 3 * i + kind
        return remote(
            conv.at[block, cut],
            conv.at[block, cut],
            conv_send.at[j],
            conv_recv.at[j],
            part=beside if kind == 0 else sibling,
        )

    for i in range(cuts):
        conv_copy(i, 1).start()
    for p in range(1, per):
        closed(p)

    units = hidden.shape[3]
    tile, steps = tiles(units, 256)

    def gather_rows(q, h):
        return arrived[q, h * per : (h + 1) * per].reshape(rows, quarter)

    def deep(q):
        return pl.ds(pl.multiple_of(q * quarter, quarter), quarter)

    def project(h, blocks, begin):
        for i in range(steps):
            span = slice(i * tile, (i + 1) * tile)
            for weight, total in ((wgate, gate_sum), (wup, up_sum)):
                value = sum(
                    jnp.dot(gather_rows(q, h), weight[deep(q), span], preferred_element_type=F32)
                    for q in blocks
                )
                total[:, span] = value if begin else total[:, span] + value

    def hid_copy(h, kind):
        block = beside if kind == 2 else tp
        j = 3 * h + kind
        return remote(
            hidden.at[h, block],
            hidden.at[h, block],
            hid_send.at[j],
            hid_recv.at[j],
            part=beside if kind == 0 else sibling,
        )

    def activate(h):
        hidden[h, tp] = (jax.nn.silu(gate_sum[...]) * up_sum[...]).astype(BF16)
        hid_copy(h, 0).start()
        hid_copy(h, 1).start()

    def from_sibling(h):
        for p in range(h * per, (h + 1) * per):
            for which in range(2):
                for far in range(2):
                    if p or which:
                        to_sibling(p, far, which).wait_recv()

    loads[4].wait()
    loads[5].wait()
    project(0, (tp, beside), True)
    for p in range(per, groups - 1):
        closed(p)
    from_sibling(0)
    project(0, (sibling, opposite), False)
    activate(0)
    closed(groups - 1)
    project(1, (tp, beside), True)
    from_sibling(1)
    project(1, (sibling, opposite), False)
    activate(1)
    for i in range(cuts):
        conv_copy(i, 0).start()

    loads[6].wait()
    wide = down_sum.shape[2]
    pieces = result.shape[1]
    span_wide = wide // pieces

    def down(h, block, span):
        depth = pl.ds(pl.multiple_of(block * units, units), units)
        return jnp.dot(hidden[h, block], wdown[depth, span], preferred_element_type=F32)

    def down_near(h):
        hid_copy(h, 1).wait_recv()
        for c in range(pieces):
            span = slice(c * span_wide, (c + 1) * span_wide)
            down_sum[h, :, span] = down(h, tp, span) + down(h, sibling, span)

    def exchange(h, c):
        return remote(
            result.at[h, c, 1], other_result.at[h, c], res_send.at[2 * h + c], res_recv.at[2 * h + c], ep=mate
        )

    def down_far(h):
        hid_copy(h, 0).wait_recv()
        hid_copy(h, 2).start()
        for c in range(pieces):
            span = slice(c * span_wide, (c + 1) * span_wide)
            total = down_sum[h, :, span] + down(h, beside, span)
            if c == 0:
                hid_copy(h, 2).wait_recv()
            total = (total + down(h, opposite, span)).astype(BF16).reshape(per, PAIR, slots, span_wide)
            for which in range(PAIR):
                result[h, c, which] = total[:, which]
            exchange(h, c).start()

    def give_back(k, c):
        p = order.index(k)
        return remote(
            summed.at[p // per, c, p % per],
            returned.at[c, k],
            ret_send.at[c * groups + k],
            ret_recv.at[c * groups + k],
            ep=backward(k),
        )

    def combine(h, c):
        exchange(h, c).wait_recv()
        for i in range(per):
            k = order[h * per + i]
            if k and c == 0:
                give_weights(k).wait_recv()
            half = weights.shape[2] // 2
            ours = arrived_weights[k, :, 0:1]
            theirs = arrived_weights[k, :, half : half + 1]
            total = ours * result[h, c, 0, i].astype(F32) + theirs * other_result[h, c, i].astype(F32)
            if k:
                summed[h, c, i] = total.astype(BF16)
                give_back(k, c).start()
            else:
                returned[c, 0] = total.astype(BF16)

    width = parts * channels
    norm_chunk, norm_chunks = tiles(share_rows, 64)

    def normalize(cut):
        @pl.loop(0, norm_chunks)
        def _(i):
            span = pl.ds(pl.multiple_of(cut * share_rows + i * norm_chunk, norm_chunk), norm_chunk)
            blocks = [conv[b, span, :].astype(F32) for b in range(parts)]
            center = sum(jnp.sum(block, axis=1, keepdims=True) for block in blocks) / width
            blocks = [block - center for block in blocks]
            spread = sum(jnp.sum(block * block, axis=1, keepdims=True) for block in blocks) / width
            scale = lax.rsqrt(spread + 1e-05)
            for b in range(parts):
                lanes = slice(b * channels, (b + 1) * channels)
                normed = blocks[b] * scale * gain_ref[:, lanes] + shift_ref[:, lanes]
                swished[b, span, :] = jax.nn.silu(normed).astype(BF16)

    out_tile, out_steps = tiles(mixer.shape[1], 256)

    def mix(cut):
        cut_rows = pl.ds(cut * share_rows, share_rows)

        @pl.loop(0, out_steps)
        def _(i):
            span = pl.ds(pl.multiple_of(i * out_tile, out_tile), out_tile)
            total = jnp.zeros((share_rows, out_tile), F32)
            for b in range(parts):
                total = total + jnp.dot(
                    swished[b, cut_rows], wout[b * channels : (b + 1) * channels, span], preferred_element_type=F32
                )
            mixer[cut_rows, span] = total.astype(BF16)

    down_near(0)
    down_far(0)
    down_near(1)
    down_far(1)
    for c in range(pieces):
        combine(0, c)
    for i in range(cuts):
        conv_copy(i, 1).wait_recv()
    conv_copy(0, 0).wait_recv()
    conv_copy(0, 2).start()
    for c in range(pieces):
        combine(1, c)
    loads[7].wait()
    conv_copy(0, 2).wait_recv()
    normalize(0)
    mix(0)
    for i in range(1, cuts):
        conv_copy(i, 0).wait_recv()
        conv_copy(i, 2).start()
    for i in range(1, cuts):
        conv_copy(i, 2).wait_recv()
        normalize(i)
        mix(i)
    for c in range(pieces):
        for k in range(1, groups):
            give_back(k, c).wait_recv()
        block = returned[c].reshape(groups * slots, span_wide)
        combined[:, c * span_wide : (c + 1) * span_wide] = jnp.dot(
            scatter[...], block, preferred_element_type=F32
        ).astype(BF16)

    for k in range(1, groups):
        dispatch(k).wait_send()
        give_weights(k).wait_send()
        for c in range(pieces):
            give_back(k, c).wait_send()
    for p in range(groups):
        if p:
            to_beside(p).wait_send()
        to_mate(p).wait_send()
        across(p).wait_send()
        for which in range(2):
            for far in range(2):
                if p or which:
                    to_sibling(p, far, which).wait_send()
    for kind in range(3):
        for i in range(cuts):
            conv_copy(i, kind).wait_send()
        for h in range(spans):
            hid_copy(h, kind).wait_send()
    for h in range(spans):
        for c in range(pieces):
            exchange(h, c).wait_send()


def pair_call(groups, parts, args):
    conv_value, expert_input, expert_gate, expert_down = args[0], args[2], args[3], args[5]
    out_weight, conv_kernel = args[6], args[7]
    channels, length = conv_value.shape
    count, model = expert_input.shape
    slots = count // groups
    quarter = model // parts
    units, wide = expert_gate.shape[2], expert_down.shape[2]
    out_width = out_weight.shape[1]
    edge = -(-((conv_kernel.shape[0] - 1) // 2) // 16) * 16
    spans, cuts, pieces = 2, 2, 2
    per = groups // spans
    rows = per * PAIR * slots
    piece = wide // pieces
    anywhere = pl.BlockSpec(memory_space=pl.ANY)
    near = pl.BlockSpec(memory_space=pltpu.VMEM)
    dma = pltpu.SemaphoreType.DMA
    return pl.pallas_call(
        functools.partial(pair_kernel, groups, parts),
        out_shape=(
            pltpu.VMEM((length, out_width), BF16),
            pltpu.VMEM((count, wide), BF16),
        ),
        in_specs=[anywhere] * 7 + [near] * 6,
        out_specs=(near, near),
        scratch_shapes=[
            pltpu.VMEM((channels, length), BF16),
            pltpu.VMEM((channels, length), BF16),
            pltpu.VMEM((count, quarter), BF16),
            pltpu.VMEM((count, model), BF16),
            pltpu.VMEM((model, units), BF16),
            pltpu.VMEM((model, units), BF16),
            pltpu.VMEM(expert_down.shape[1:], BF16),
            pltpu.VMEM(out_weight.shape, BF16),
            pltpu.VMEM((groups - 1, slots, quarter), BF16),
            pltpu.VMEM((groups, slots, 128), F32),
            pltpu.VMEM((groups, slots, 128), F32),
            pltpu.VMEM((parts, groups, PAIR, slots, quarter), BF16),
            pltpu.VMEM((rows, units), F32),
            pltpu.VMEM((rows, units), F32),
            pltpu.VMEM((spans, parts, rows, units), BF16),
            pltpu.VMEM((spans, rows, wide), F32),
            pltpu.VMEM((spans, pieces, PAIR, per, slots, piece), BF16),
            pltpu.VMEM((spans, pieces, per, slots, piece), BF16),
            pltpu.VMEM((spans, pieces, per, slots, piece), BF16),
            pltpu.VMEM((pieces, groups, slots, piece), BF16),
            pltpu.VMEM((count, groups * slots), BF16),
            pltpu.VMEM((length + 2 * edge, channels), F32),
            pltpu.VMEM((2, edge, channels), BF16),
            pltpu.VMEM((2, edge, channels), BF16),
            pltpu.VMEM((parts, length, channels), BF16),
            pltpu.VMEM((parts, length, channels), BF16),
            dma((8,)),
            dma((groups,)),
            dma((groups,)),
            dma((groups,)),
            dma((groups,)),
            dma((groups,)),
            dma((groups,)),
            dma((groups,)),
            dma((groups,)),
            dma((groups,)),
            dma((groups,)),
            dma((4 * groups,)),
            dma((4 * groups,)),
            dma((2,)),
            dma((2,)),
            dma((3 * cuts,)),
            dma((3 * cuts,)),
            dma((3 * spans,)),
            dma((3 * spans,)),
            dma((spans * pieces,)),
            dma((spans * pieces,)),
            dma((pieces * groups,)),
            dma((pieces * groups,)),
        ],
        compiler_params=pltpu.CompilerParams(
            collective_id=0, has_side_effects=True, vmem_limit_bytes=60 * 1024 * 1024
        ),
        name="pair_block",
    )(*args)


def local(
    experts,
    parts,
    conv_value,
    conv_gate,
    conv_kernel,
    norm_gain,
    norm_shift,
    out_weight,
    expert_input,
    expert_ids,
    pair_logits,
    group_prob,
    expert_gate,
    expert_up,
    expert_down,
):
    channels, length = conv_value.shape
    count, model = expert_input.shape
    slots = 2 * count // experts
    rows = experts * slots
    half = model // CORES
    units, wide = expert_gate.shape[2], expert_down.shape[2]
    out_width = out_weight.shape[1]
    chips = parts // CORES
    args = (
        conv_value,
        conv_gate,
        expert_input,
        expert_gate,
        expert_up,
        expert_down,
        out_weight,
        conv_kernel,
        norm_gain[None, :],
        norm_shift[None, :],
        expert_ids.T,
        pair_logits.T,
        group_prob[None, :],
    )
    if experts == GROUPS * PAIR and chips == 2:
        return pair_call(GROUPS, parts, args)
    edge = -(-((conv_kernel.shape[0] - 1) // 2) // 16) * 16
    anywhere = pl.BlockSpec(memory_space=pl.ANY)
    near = pl.BlockSpec(memory_space=pltpu.VMEM)
    dma = pltpu.SemaphoreType.DMA
    return pl.pallas_call(
        functools.partial(kernel, experts, parts),
        out_shape=(
            pltpu.VMEM((length, out_width), BF16),
            pltpu.VMEM((count, wide), BF16),
        ),
        in_specs=[anywhere] * 7 + [near] * 6,
        out_specs=(anywhere, anywhere),
        scratch_shapes=[
            pltpu.VMEM((channels, length), BF16),
            pltpu.VMEM((channels, length), BF16),
            pltpu.VMEM((count, half), BF16),
            pltpu.VMEM((model, units), BF16),
            pltpu.VMEM((model, units), BF16),
            pltpu.VMEM(expert_down.shape[1:], BF16),
            pltpu.VMEM(out_weight.shape, BF16),
            pltpu.VMEM((experts, slots, half), BF16),
            pltpu.VMEM((CORES, experts, slots, half), BF16),
            pltpu.VMEM((rows, units), F32),
            pltpu.VMEM((rows, units), F32),
            pltpu.VMEM((parts, rows, units), BF16),
            pltpu.VMEM((rows, wide), F32),
            pltpu.VMEM((experts, slots, wide), BF16),
            pltpu.VMEM((experts, slots, wide), BF16),
            pltpu.VMEM((length + 2 * edge, channels), F32),
            pltpu.VMEM((2, edge, channels), BF16),
            pltpu.VMEM((2, edge, channels), BF16),
            pltpu.VMEM((parts, length, channels), BF16),
            pltpu.VMEM((parts, length, channels), BF16),
            pltpu.VMEM((length, out_width), BF16),
            pltpu.VMEM((count, wide), BF16),
            dma((7,)),
            dma((2,)),
            dma((2,)),
            dma((experts,)),
            dma((experts,)),
            dma((experts,)),
            dma((experts,)),
            dma((2,)),
            dma((2,)),
            dma((2 * chips,)),
            dma((2 * chips,)),
            dma((2 * chips,)),
            dma((2 * chips,)),
            dma((experts,)),
            dma((experts,)),
        ],
        compiler_params=pltpu.CompilerParams(
            collective_id=0, has_side_effects=True, vmem_limit_bytes=60 * 1024 * 1024
        ),
        name="block",
    )(*args)

def solution(mesh):
    placed = (
        P("tp", "ep"),
        P("tp", "ep"),
        P(None, "tp"),
        P(),
        P(),
        P(None, "tp"),
        P("ep", None),
        P("ep", None),
        P("ep", None),
        P("ep"),
        P("ep", None, "tp"),
        P("ep", None, "tp"),
        P("ep", None, "tp"),
    )
    return jax.shard_map(
        functools.partial(local, mesh.shape["ep"], mesh.shape["tp"]),
        mesh=mesh,
        in_specs=placed,
        out_specs=(P("ep", "tp"), P("ep", "tp")),
        check_vma=False,
    )
```

```python
import functools

import jax
import jax.numpy as jnp
from jax import lax
from jax.experimental import pallas as pl
from jax.experimental.pallas import tpu as pltpu
from jax.sharding import PartitionSpec as P

MESH = pl.DeviceIdType.MESH
CORES = 2
PAIR = 2
GROUPS = 4
F32, BF16 = jnp.float32, jnp.bfloat16


def tiles(size, most):
    tile = min(size, most)
    return tile, size // tile


def kernel(
    experts,
    parts,
    value_hbm,
    gate_hbm,
    input_hbm,
    wgate_hbm,
    wup_hbm,
    wdown_hbm,
    wout_hbm,
    taps_ref,
    gain_ref,
    shift_ref,
    ids_ref,
    logits_ref,
    prob_ref,
    mixer_hbm,
    expert_hbm,
    value,
    gate,
    tokens,
    wgate,
    wup,
    wdown,
    wout,
    send_rows,
    arrived,
    gate_sum,
    up_sum,
    hidden,
    down_sum,
    result,
    returned,
    padded,
    edges,
    halo,
    conv,
    swished,
    mixer,
    combined,
    load_sem,
    out_sem,
    self_sem,
    disp_send,
    disp_recv,
    fwd_send,
    fwd_recv,
    hal_send,
    hal_recv,
    conv_send,
    conv_recv,
    hid_send,
    hid_recv,
    ret_send,
    ret_recv,
):
    me = lax.axis_index("ep")
    tp = lax.axis_index("tp")
    chips = parts // CORES
    chip, core = lax.div(tp, CORES), lax.rem(tp, CORES)
    other = 1 - core
    sibling = chip * CORES + other
    slots = send_rows.shape[1]
    half = send_rows.shape[2]
    rows = experts * slots
    length, channels = conv.shape[1], conv.shape[2]
    edge = halo.shape[1]
    reach = (taps_ref.shape[0] - 1) // 2

    def remote(src, dst, ssem, rsem, ep=None, part=None):
        target = (me if ep is None else ep, tp if part is None else part)
        return pltpu.make_async_remote_copy(
            src_ref=src, dst_ref=dst, send_sem=ssem, recv_sem=rsem, device_id=target, device_id_type=MESH
        )

    def ahead(k):
        return lax.rem(me + k, experts)

    def behind(k):
        return lax.rem(me + experts - k, experts)

    def chip_ahead(k):
        return lax.rem(chip + k, chips) * CORES + core

    def chip_behind(k):
        return lax.rem(chip + chips - k, chips) * CORES + core

    barrier = pltpu.get_barrier_semaphore()

    @pl.loop(1, experts)
    def _(k):
        pl.semaphore_signal(barrier, inc=1, device_id=(ahead(k), tp), device_id_type=MESH)

    @pl.loop(1, chips)
    def _(k):
        pl.semaphore_signal(barrier, inc=1, device_id=(me, chip_ahead(k)), device_id_type=MESH)

    pl.semaphore_signal(barrier, inc=1, device_id=(me, sibling), device_id_type=MESH)

    columns = pl.ds(pl.multiple_of(core * half, half), half)
    loads = [
        pltpu.make_async_copy(src, dst, load_sem.at[i])
        for i, (src, dst) in enumerate(
            [
                (input_hbm.at[:, columns], tokens),
                (value_hbm, value),
                (gate_hbm, gate),
                (wgate_hbm.at[0], wgate),
                (wup_hbm.at[0], wup),
                (wout_hbm, wout),
                (wdown_hbm.at[0], wdown),
            ]
        )
    ]
    for load in loads:
        load.start()

    count = ids_ref.shape[1]
    first, second = ids_ref[0:1, :], ids_ref[1:2, :]
    expert_of = lax.broadcasted_iota(jnp.int32, (experts, count), 0)
    is_first, is_second = expert_of == first, expert_of == second
    chosen = jnp.where(is_first | is_second, 1.0, 0.0).astype(F32)
    earlier = lax.broadcasted_iota(jnp.int32, (count, count), 0) < lax.broadcasted_iota(
        jnp.int32, (count, count), 1
    )
    rank = jnp.dot(
        chosen.astype(BF16), jnp.where(earlier, 1.0, 0.0).astype(BF16), preferred_element_type=F32
    )
    rank = jnp.where(chosen > 0, rank, -1.0)
    ordinal = lax.broadcasted_iota(jnp.int32, (experts, slots, count), 1).astype(F32)
    place3 = jnp.broadcast_to(rank[:, None, :], (experts, slots, count)) == ordinal
    place = jnp.where(place3, 1.0, 0.0).astype(F32).reshape(rows, count)

    loads[0].wait()
    tile, steps = tiles(half, 512)
    for i in range(steps):
        span = slice(i * tile, (i + 1) * tile)
        picked = jnp.dot(place.astype(BF16), tokens[:, span], preferred_element_type=F32)
        send_rows[:, :, span] = picked.reshape(experts, slots, tile).astype(BF16)

    pl.semaphore_wait(barrier, experts - 1 + chips)

    def dispatch(k):
        return remote(
            send_rows.at[ahead(k)], arrived.at[core, me], disp_send.at[k], disp_recv.at[k], ep=ahead(k)
        )

    def forward(k, src):
        return remote(
            src, arrived.at[core, behind(k)], fwd_send.at[k], fwd_recv.at[k], part=sibling
        )

    @pl.loop(1, experts)
    def _(k):
        dispatch(k).start()

    keep = pltpu.make_async_copy(send_rows.at[me], arrived.at[core, me], self_sem.at[0])
    keep.start()
    forward(0, send_rows.at[me]).start()

    loads[1].wait()
    loads[2].wait()
    gated = (value[...].astype(F32) * jax.nn.sigmoid(gate[...].astype(F32))).astype(BF16)
    padded[edge : edge + length, :] = jnp.transpose(gated.astype(F32), (1, 0))
    edges[0] = padded[edge : 2 * edge, :].astype(BF16)
    edges[1] = padded[length : length + edge, :].astype(BF16)
    to_left = remote(edges.at[0], halo.at[1], hal_send.at[0], hal_recv.at[0], ep=behind(1))
    to_right = remote(edges.at[1], halo.at[0], hal_send.at[1], hal_recv.at[1], ep=ahead(1))
    to_left.start()
    to_right.start()
    taps = taps_ref[...].astype(F32)
    chunk, chunks = tiles(length, 64)

    def convolve(i):
        total = jnp.zeros((chunk, channels), F32)
        for j in range(taps.shape[0]):
            start = i * chunk + j + edge - reach
            total = total + taps[j : j + 1, :] * padded[start : start + chunk, :]
        conv[tp, i * chunk : (i + 1) * chunk, :] = total.astype(BF16)

    for i in range(1, chunks - 1):
        convolve(i)
    to_left.wait()
    to_right.wait()
    padded[0:edge, :] = jnp.where(me == 0, 0.0, halo[0].astype(F32))
    padded[edge + length : 2 * edge + length, :] = jnp.where(
        me == experts - 1, 0.0, halo[1].astype(F32)
    )
    convolve(0)
    convolve(chunks - 1)

    def gather(buffer, ssem, rsem):
        def across(k):
            return remote(buffer.at[tp], buffer.at[tp], ssem.at[k], rsem.at[k], part=chip_ahead(k))

        def beside(k):
            block = chip_behind(k)
            return remote(
                buffer.at[block], buffer.at[block], ssem.at[chips + k], rsem.at[chips + k], part=sibling
            )

        return across, beside

    conv_across, conv_beside = gather(conv, conv_send, conv_recv)

    @pl.loop(1, chips)
    def _(k):
        conv_across(k).start()

    conv_beside(0).start()

    @pl.loop(1, experts)
    def _(k):
        dispatch(k).wait_recv()
        forward(k, arrived.at[core, behind(k)]).start()

    keep.wait()
    loads[3].wait()
    loads[4].wait()
    units = gate_sum.shape[1]
    tile, steps = tiles(units, 256)

    def side(which):
        block = arrived[which]
        if slots % 16:
            return block.astype(F32).reshape(rows, half).astype(BF16)
        return block.reshape(rows, half)

    def depth(which):
        return pl.ds(pl.multiple_of(which * half, half), half)

    for i in range(steps):
        span = slice(i * tile, (i + 1) * tile)
        gate_sum[:, span] = jnp.dot(side(core), wgate[depth(core), span], preferred_element_type=F32)
        up_sum[:, span] = jnp.dot(side(core), wup[depth(core), span], preferred_element_type=F32)

    @pl.loop(0, experts)
    def _(k):
        forward(k, send_rows.at[me]).wait_recv()

    for i in range(steps):
        span = slice(i * tile, (i + 1) * tile)
        gate_val = gate_sum[:, span] + jnp.dot(
            side(other), wgate[depth(other), span], preferred_element_type=F32
        )
        up_val = up_sum[:, span] + jnp.dot(
            side(other), wup[depth(other), span], preferred_element_type=F32
        )
        hidden[tp, :, span] = (jax.nn.silu(gate_val) * up_val).astype(BF16)

    hid_across, hid_beside = gather(hidden, hid_send, hid_recv)

    @pl.loop(1, chips)
    def _(k):
        hid_across(k).start()

    hid_beside(0).start()

    @pl.loop(1, chips)
    def _(k):
        conv_across(k).wait_recv()
        conv_beside(k).start()

    @pl.loop(0, chips)
    def _(k):
        conv_beside(k).wait_recv()

    width = parts * channels
    chunk, chunks = tiles(length, 64)

    @pl.loop(0, chunks)
    def _(i):
        span = pl.ds(pl.multiple_of(i * chunk, chunk), chunk)
        blocks = [conv[b, span, :].astype(F32) for b in range(parts)]
        center = sum(jnp.sum(block, axis=1, keepdims=True) for block in blocks) / width
        blocks = [block - center for block in blocks]
        spread = sum(jnp.sum(block * block, axis=1, keepdims=True) for block in blocks) / width
        scale = lax.rsqrt(spread + 1e-05)
        for b in range(parts):
            lanes = slice(b * channels, (b + 1) * channels)
            normed = blocks[b] * scale * gain_ref[:, lanes] + shift_ref[:, lanes]
            swished[b, span, :] = jax.nn.silu(normed).astype(BF16)

    loads[6].wait()
    wide = down_sum.shape[1]
    tile, steps = tiles(wide, 256)

    def down(block, begin):
        deep = pl.ds(pl.multiple_of(block * units, units), units)

        @pl.loop(0, steps)
        def _(i):
            span = pl.ds(pl.multiple_of(i * tile, tile), tile)
            product = jnp.dot(hidden[block], wdown[deep, span], preferred_element_type=F32)
            down_sum[:, span] = product if begin else down_sum[:, span] + product

    down(tp, True)
    hid_beside(0).wait_recv()
    down(sibling, False)

    @pl.loop(1, chips)
    def _(k):
        hid_across(k).wait_recv()
        hid_beside(k).start()
        down(chip_behind(k), False)
        hid_beside(k).wait_recv()
        down(chip_behind(k) + other - core, False)

    result[...] = down_sum[...].reshape(experts, slots, wide).astype(BF16)

    def give_back(k):
        return remote(result.at[ahead(k)], returned.at[me], ret_send.at[k], ret_recv.at[k], ep=ahead(k))

    @pl.loop(1, experts)
    def _(k):
        give_back(k).start()

    own = pltpu.make_async_copy(result.at[me], returned.at[me], self_sem.at[1])
    own.start()

    loads[5].wait()
    tile, steps = tiles(mixer.shape[1], 256)

    @pl.loop(0, steps)
    def _(i):
        span = pl.ds(pl.multiple_of(i * tile, tile), tile)
        total = jnp.zeros((length, tile), F32)
        for b in range(parts):
            total = total + jnp.dot(
                swished[b], wout[b * channels : (b + 1) * channels, span], preferred_element_type=F32
            )
        mixer[:, span] = total.astype(BF16)

    put_mixer = pltpu.make_async_copy(mixer, mixer_hbm, out_sem.at[0])
    put_mixer.start()

    share = jax.nn.sigmoid(logits_ref[0:1, :] - logits_ref[1:2, :])
    weight = jnp.where(is_first, share * prob_ref[...], 0.0) + jnp.where(
        is_second, (1.0 - share) * prob_ref[...], 0.0
    )
    weights = jnp.where(
        place3, jnp.broadcast_to(weight[:, None, :], (experts, slots, count)), 0.0
    ).reshape(rows, count)
    weights = jnp.transpose(weights, (1, 0))
    high = weights.astype(BF16)
    rest = weights - high.astype(F32)
    middle = rest.astype(BF16)
    low = (rest - middle.astype(F32)).astype(BF16)

    own.wait()

    @pl.loop(1, experts)
    def _(k):
        give_back(k).wait_recv()

    tile, steps = tiles(wide, 512)
    for i in range(steps):
        span = slice(i * tile, (i + 1) * tile)
        block = returned[:, :, span]
        if slots % 16:
            block = block.astype(F32).reshape(rows, tile).astype(BF16)
        else:
            block = block.reshape(rows, tile)
        total = jnp.dot(low, block, preferred_element_type=F32)
        total = total + jnp.dot(middle, block, preferred_element_type=F32)
        total = total + jnp.dot(high, block, preferred_element_type=F32)
        combined[:, span] = total.astype(BF16)

    put_expert = pltpu.make_async_copy(combined, expert_hbm, out_sem.at[1])
    put_expert.start()

    @pl.loop(1, experts)
    def _(k):
        dispatch(k).wait_send()
        give_back(k).wait_send()

    @pl.loop(0, experts)
    def _(k):
        forward(k, send_rows.at[me]).wait_send()

    @pl.loop(1, chips)
    def _(k):
        conv_across(k).wait_send()
        hid_across(k).wait_send()

    @pl.loop(0, chips)
    def _(k):
        conv_beside(k).wait_send()
        hid_beside(k).wait_send()

    put_mixer.wait()
    put_expert.wait()


def pair_kernel(
    groups,
    parts,
    value_hbm,
    gate_hbm,
    input_hbm,
    wgate_hbm,
    wup_hbm,
    wdown_hbm,
    wout_hbm,
    taps_hbm,
    gain_hbm,
    shift_hbm,
    ids_hbm,
    logits_hbm,
    prob_hbm,
    mixer,
    combined,
    taps_ref,
    affine,
    ids_ref,
    logits_ref,
    prob_ref,
    values,
    mine,
    tokens,
    projections,
    wdown,
    wout,
    send_rows,
    weights,
    arrived_weights,
    arrived,
    gate_sum,
    up_sum,
    hidden,
    down_sum,
    result,
    other_result,
    summed,
    returned,
    scatter,
    padded,
    edges,
    halo,
    conv,
    stats,
    swished,
    load_sem,
    z_send,
    z_recv,
    w_send,
    w_recv,
    y_send,
    y_recv,
    x_send,
    x_recv,
    d_recv,
    s_send,
    s_recv,
    hal_send,
    hal_recv,
    stat_send,
    stat_recv,
    mix_send,
    mix_recv,
    hid_send,
    hid_recv,
    res_send,
    res_recv,
    ret_send,
    ret_recv,
):
    experts = groups * PAIR
    me = lax.axis_index("ep")
    tp = lax.axis_index("tp")
    group, side = lax.div(me, PAIR), lax.rem(me, PAIR)
    mate = group * PAIR + 1 - side
    chip, core = lax.div(tp, CORES), lax.rem(tp, CORES)
    sibling = chip * CORES + 1 - core
    beside = (1 - chip) * CORES + core
    opposite = (1 - chip) * CORES + 1 - core
    slots, quarter = send_rows.shape[1], send_rows.shape[2]
    blocks = [(0, groups // 2)] + [(p, 1) for p in range(groups // 2, groups)]
    each = PAIR * slots
    straight = (1,)
    length, channels = conv.shape
    edge = halo.shape[1]
    reach = (taps_ref.shape[0] - 1) // 2

    def remote(src, dst, ssem, rsem, ep=None, part=None):
        target = (me if ep is None else ep, tp if part is None else part)
        return pltpu.make_async_remote_copy(
            src_ref=src, dst_ref=dst, send_sem=ssem, recv_sem=rsem, device_id=target, device_id_type=MESH
        )

    def onward(k):
        return lax.rem(group + k, groups) * PAIR + side

    def backward(k):
        return lax.rem(group + groups - k, groups) * PAIR + side

    left, right = lax.rem(me + experts - 1, experts), lax.rem(me + 1, experts)
    barrier = pltpu.get_barrier_semaphore()
    peers = [(onward(k), tp) for k in range(1, groups)]
    peers += [(mate, tp), (me, beside), (me, sibling), (me, opposite), (mate, beside), (left, tp), (right, tp)]
    for peer in peers:
        pl.semaphore_signal(barrier, inc=1, device_id=peer, device_id_type=MESH)

    columns = pl.ds(pl.multiple_of(tp * quarter, quarter), quarter)
    def load(i, *pairs):
        return [pltpu.make_async_copy(src, dst, load_sem.at[i]) for src, dst in pairs]

    loads = [
        load(0, (ids_hbm, ids_ref)),
        load(1, (input_hbm.at[:, columns], mine)),
        load(2, (logits_hbm, logits_ref)),
        load(3, (prob_hbm, prob_ref)),
        load(4, (input_hbm, tokens)),
        load(5, (value_hbm, values.at[0]), (gate_hbm, values.at[1])),
        load(6, (taps_hbm, taps_ref)),
        load(7, (wgate_hbm, projections.at[0:1]), (wup_hbm, projections.at[1:2])),
        load(8, (wdown_hbm.at[0], wdown)),
        load(9, (wout_hbm, wout)),
        load(10, (gain_hbm, affine.at[0]), (shift_hbm, affine.at[1])),
    ]
    for copies in loads:
        for copy in copies:
            copy.start()

    def loaded(i):
        whole = {5: values, 7: projections, 10: affine}.get(i)
        if whole is None:
            loads[i][0].wait()
        else:
            pltpu.make_async_copy(whole, whole, load_sem.at[i]).wait()

    loaded(0)

    count = ids_ref.shape[1]
    first, second = ids_ref[0:1, :], ids_ref[1:2, :]
    position = lax.broadcasted_iota(jnp.int32, (groups, count), 0) + group
    position = jnp.where(position >= groups, position - groups, position) * PAIR
    chosen = jnp.where((first >= position) & (first < position + PAIR), 1.0, 0.0).astype(F32)
    earlier = lax.broadcasted_iota(jnp.int32, (count, count), 0) < lax.broadcasted_iota(
        jnp.int32, (count, count), 1
    )
    rank = jnp.dot(
        chosen.astype(BF16), jnp.where(earlier, 1.0, 0.0).astype(BF16), preferred_element_type=F32
    )
    rank = jnp.where(chosen > 0, rank, -1.0)
    ordinal = lax.broadcasted_iota(jnp.int32, (groups, slots, count), 1).astype(F32)
    place3 = jnp.broadcast_to(rank[:, None, :], (groups, slots, count)) == ordinal
    place_f = jnp.where(place3, 1.0, 0.0).astype(F32).reshape(groups * slots, count)
    place = place_f.astype(BF16)

    def dispatch(k):
        return remote(
            send_rows.at[k - 1],
            arrived.at[tp, k, 0],
            z_send.at[0],
            z_recv.at[k],
            ep=onward(k),
        )

    loaded(1)
    picked = jnp.dot(place[slots:], mine[...], preferred_element_type=F32)
    send_rows[...] = picked.astype(BF16).reshape(groups - 1, slots, quarter)
    pl.semaphore_wait(barrier, len(peers))
    for k in range(1, groups):
        dispatch(k).start()

    def to_beside(p):
        return remote(
            arrived.at[tp, p, 0], arrived.at[tp, p, 0], y_send.at[0], y_recv.at[p], part=beside
        )

    def to_mate(p):
        return remote(arrived.at[tp, p, 0], arrived.at[tp, p, 1], x_send.at[0], x_recv.at[p], ep=mate)

    def across(p):
        if p == 0:
            return remote(
                arrived.at[beside, 0, 0], arrived.at[beside, 0, 1], x_send.at[0], d_recv.at[0], ep=mate
            )
        if p in straight:
            return remote(
                arrived.at[tp, p, 0], arrived.at[tp, p, 1], x_send.at[0], d_recv.at[p], ep=mate, part=beside
            )
        return remote(
            arrived.at[beside, p, 0], arrived.at[beside, p, 1], x_send.at[0], d_recv.at[p], ep=mate
        )

    def to_sibling(p, far, which):
        block = beside if far else tp
        return remote(
            arrived.at[block, p, which],
            arrived.at[block, p, which],
            s_send.at[min(p, 1)],
            s_recv.at[sum(start <= p for start, _ in blocks) - 1],
            part=sibling,
        )

    def all_sent(whole, sem):
        remote(whole, whole, sem, sem, part=sibling).wait_send()

    def all_received(whole, sem):
        remote(whole, whole, sem, sem, part=sibling).wait_recv()

    loaded(4)
    for q in range(parts):
        picked = jnp.dot(
            place[:slots], tokens[:, q * quarter : (q + 1) * quarter], preferred_element_type=F32
        )
        arrived[q, 0, 0] = picked.astype(BF16)
    to_mate(0).start()
    across(0).start()

    loaded(2)
    loaded(3)
    share = jax.nn.sigmoid(logits_ref[0:1, :] - logits_ref[1:2, :])
    of_first = share * prob_ref[...]
    of_second = (1.0 - share) * prob_ref[...]
    first_mine = (first < second) == (side == 0)
    own_weight = jnp.sum(place_f * jnp.where(first_mine, of_first, of_second), axis=1, keepdims=True)
    mate_weight = jnp.sum(place_f * jnp.where(first_mine, of_second, of_first), axis=1, keepdims=True)
    lane = lax.broadcasted_iota(jnp.int32, (groups * slots, weights.shape[2]), 1)
    both = jnp.where(lane < weights.shape[2] // 2, own_weight, mate_weight)
    weights[...] = both.reshape(weights.shape)

    def give_weights(k):
        return remote(weights.at[k], arrived_weights.at[k], w_send.at[0], w_recv.at[0], ep=onward(k))

    arrived_weights[0] = weights[0]
    scatter[...] = jnp.transpose(place_f, (1, 0)).astype(BF16)

    loaded(5)
    loaded(6)
    gated = (values[0].astype(F32) * jax.nn.sigmoid(values[1].astype(F32))).astype(BF16)
    padded[edge : edge + length, :] = jnp.transpose(gated.astype(F32), (1, 0))
    edges[0] = padded[edge : 2 * edge, :].astype(BF16)
    edges[1] = padded[length : length + edge, :].astype(BF16)
    to_left = remote(edges.at[0], halo.at[1], hal_send.at[0], hal_recv.at[0], ep=left)
    to_right = remote(edges.at[1], halo.at[0], hal_send.at[0], hal_recv.at[0], ep=right)
    to_left.start()
    to_right.start()
    for k in range(1, groups):
        give_weights(k).start()
    taps = taps_ref[...].astype(F32)
    chunk, chunks = tiles(length, 64)

    def convolve(i):
        total = jnp.zeros((chunk, channels), F32)
        for j in range(taps.shape[0]):
            start = i * chunk + j + edge - reach
            total = total + taps[j : j + 1, :] * padded[start : start + chunk, :]
        conv[i * chunk : (i + 1) * chunk, :] = total.astype(BF16)

    def landed(p):
        dispatch(p).wait_recv()
        to_beside(p).start()
        to_mate(p).start()
        if p in straight:
            across(p).start()
        to_sibling(p, 0, 0).start()

    def turned(p):
        if p:
            to_beside(p).wait_recv()
            if p not in straight:
                across(p).start()
            to_sibling(p, 1, 0).start()
        to_mate(p).wait_recv()
        to_sibling(p, 0, 1).start()

    def closed(p):
        across(p).wait_recv()
        to_sibling(p, 1, 1).start()

    def measure():
        block = conv[...].astype(F32)
        center = jnp.sum(block, axis=1, keepdims=True) / channels
        block = block - center
        spread = jnp.sum(block * block, axis=1, keepdims=True)
        lane = lax.broadcasted_iota(jnp.int32, (length, 128), 1)
        turned_over = jnp.transpose(jnp.where(lane == 0, center, spread), (1, 0))
        lanes = stats.shape[2]
        for i in range(length // lanes):
            span = slice(i * lanes, (i + 1) * lanes)
            stats[tp, i : i + 1] = turned_over[0:1, span]
            stats[tp, i + length // lanes : i + 1 + length // lanes] = turned_over[1:2, span]
        for i in range(3):
            tell(i).start()

    def tell(i):
        part = (sibling, beside, opposite)[i]
        return remote(stats.at[tp], stats.at[tp], stat_send.at[0], stat_recv.at[0], part=part)

    def normalize():
        all_received(stats.at[0:3], stat_recv.at[0])
        wraps = length // stats.shape[2]
        centers = [stats[b, 0:wraps] for b in range(parts)]
        center = sum(centers) / parts
        spread = sum(
            stats[b, wraps : 2 * wraps] + channels * jnp.square(centers[b] - center) for b in range(parts)
        )
        scale = lax.rsqrt(spread / (parts * channels) + 1e-05)
        row = lax.broadcasted_iota(jnp.int32, (128, stats.shape[2]), 0)
        turned_over = [
            jnp.transpose(jnp.where(row == 0, center[i : i + 1], scale[i : i + 1]), (1, 0)) for i in range(wraps)
        ]
        across_rows = jnp.concatenate(turned_over, axis=0)
        center, scale = across_rows[:, 0:1], across_rows[:, 1:2]
        lanes = pl.ds(pl.multiple_of(tp * channels, channels), channels)
        normed = (conv[...].astype(F32) - center) * scale * affine[0, :, lanes] + affine[1, :, lanes]
        swished[tp] = jax.nn.silu(normed).astype(BF16)

    cuts = mix_recv.shape[0] // 2
    share_rows = length // cuts

    def share_copy(i, kind):
        cut = pl.ds(i * share_rows, share_rows)
        block = beside if kind == 2 else tp
        j = 2 * cuts if kind == 1 else 2 * i + kind // 2
        return remote(
            swished.at[block, cut],
            swished.at[block, cut],
            mix_send.at[0],
            mix_recv.at[j],
            part=beside if kind == 0 else sibling,
        )

    units = hidden.shape[2]
    tile, steps = tiles(units, 256)

    def extent(h):
        start, size = blocks[h]
        return slice(start * each, (start + size) * each)

    def deep(q):
        return pl.ds(pl.multiple_of(q * quarter, quarter), quarter)

    def project(h, quarters, begin):
        start, size = blocks[h]
        for i in range(steps):
            span = slice(i * tile, (i + 1) * tile)
            for which, total in enumerate((gate_sum, up_sum)):
                product = sum(
                    jnp.dot(
                        arrived[q, start : start + size].reshape(size * each, quarter),
                        projections[which, deep(q), span],
                        preferred_element_type=F32,
                    )
                    for q in quarters
                )
                total[extent(h), span] = product if begin else total[extent(h), span] + product

    def hid_copy(h, kind):
        block = beside if kind == 2 else tp
        j = 3 * h + kind
        return remote(
            hidden.at[block, extent(h)],
            hidden.at[block, extent(h)],
            hid_send.at[0],
            hid_recv.at[j],
            part=beside if kind == 0 else sibling,
        )

    def near(h):
        project(h, (tp, beside), True)

    def far(h):
        start, size = blocks[h]
        whole = arrived.at[0:2, start : start + size] if start else arrived.at[0 : 2 * size - 1, 0]
        all_received(whole, s_recv.at[h])
        project(h, (sibling, opposite), False)
        hidden[tp, extent(h)] = (jax.nn.silu(gate_sum[extent(h)]) * up_sum[extent(h)]).astype(BF16)
        hid_copy(h, 0).start()
        hid_copy(h, 1).start()

    wide = down_sum.shape[1]
    pieces = result.shape[0]
    span_wide = wide // pieces
    cols = [slice(c * span_wide, (c + 1) * span_wide) for c in range(pieces)]

    def down(h, block, c):
        depth = pl.ds(pl.multiple_of(block * units, units), units)
        return jnp.dot(hidden[block, extent(h)], wdown[depth, cols[c]], preferred_element_type=F32)

    def down_near(h):
        hid_copy(h, 1).wait_recv()
        for c in range(pieces):
            down_sum[extent(h), cols[c]] = down(h, tp, c) + down(h, sibling, c)

    def hand_on(h):
        hid_copy(h, 0).wait_recv()
        hid_copy(h, 2).start()

    def exchange(h, c):
        start, size = blocks[h]
        return remote(
            result.at[c, 1, start : start + size],
            other_result.at[c, start : start + size],
            res_send.at[0],
            res_recv.at[pieces * h + c],
            ep=mate,
        )

    def down_far(h):
        start, size = blocks[h]
        for c in range(pieces):
            down_sum[extent(h), cols[c]] += down(h, beside, c)
        hid_copy(h, 2).wait_recv()
        for c in range(pieces):
            total = (down_sum[extent(h), cols[c]] + down(h, opposite, c)).astype(BF16)
            total = total.reshape(size, PAIR, slots, span_wide)
            for which in range(PAIR):
                result[c, which, start : start + size] = total[:, which]
            exchange(h, c).start()

    def give_back(k, c):
        return remote(summed.at[c, k], returned.at[c, k], ret_send.at[0], ret_recv.at[c], ep=backward(k))

    def combine(h, c):
        if h == 0 and c == 0:
            all_received(arrived_weights.at[1:groups], w_recv.at[0])
        exchange(h, c).wait_recv()
        start, size = blocks[h]
        for k in range(start, start + size):
            middle = weights.shape[2] // 2
            ours = arrived_weights[k, :, 0:1]
            theirs = arrived_weights[k, :, middle : middle + 1]
            total = ours * result[c, 0, k].astype(F32) + theirs * other_result[c, k].astype(F32)
            if k:
                summed[c, k] = total.astype(BF16)
                give_back(k, c).start()
            else:
                returned[c, 0] = total.astype(BF16)

    out_tile, out_steps = tiles(mixer.shape[1], 256)

    def mix(cut):
        cut_rows = pl.ds(cut * share_rows, share_rows)

        for i in range(out_steps):
            span = slice(i * out_tile, (i + 1) * out_tile)
            total = sum(
                jnp.dot(swished[b, cut_rows], wout[b * channels : (b + 1) * channels, span], preferred_element_type=F32)
                for b in range(parts)
            )
            mixer[cut_rows, span] = total.astype(BF16)

    def passed(i):
        share_copy(i, 0).wait_recv()
        share_copy(i, 2).start()

    def mixed(i):
        if i == 0:
            all_received(swished.at[0], mix_recv.at[2 * cuts])
        share_copy(i, 2).wait_recv()
        mix(i)

    def combined_block(h):
        for c in range(pieces):
            combine(h, c)

    for i in range(1, chunks - 1):
        convolve(i)
    landed(1)
    turned(0)
    closed(0)
    landed(2)
    landed(3)
    turned(1)
    all_received(halo, hal_recv.at[0])
    padded[0:edge, :] = jnp.where(me == 0, 0.0, halo[0].astype(F32))
    padded[edge + length : 2 * edge + length, :] = jnp.where(
        me == experts - 1, 0.0, halo[1].astype(F32)
    )
    convolve(0)
    convolve(chunks - 1)
    measure()
    closed(1)
    loaded(7)
    near(0)
    turned(2)
    far(0)
    turned(3)
    loaded(8)
    down_near(0)
    loaded(10)
    normalize()
    for i in range(cuts):
        share_copy(i, 1).start()
    closed(2)
    near(1)
    far(1)
    closed(3)
    near(2)
    hand_on(0)
    far(2)
    for i in range(cuts):
        share_copy(i, 0).start()
    down_far(0)
    down_near(1)
    hand_on(1)
    down_near(2)
    down_far(1)
    hand_on(2)
    combine(0, 0)
    down_far(2)
    for c in range(1, pieces):
        combine(0, c)
    combined_block(1)
    passed(0)
    combined_block(2)
    loaded(9)
    mixed(0)
    for i in range(1, cuts):
        passed(i)
        mixed(i)
    for c in range(pieces):
        all_received(returned.at[c, 1:groups], ret_recv.at[c])
        block = returned[c].reshape(groups * slots, span_wide)
        combined[:, c * span_wide : (c + 1) * span_wide] = jnp.dot(
            scatter[...], block, preferred_element_type=F32
        ).astype(BF16)

    all_sent(send_rows, z_send.at[0])
    all_sent(weights.at[1:groups], w_send.at[0])
    all_sent(arrived.at[0, 1:groups, 0], y_send.at[0])
    all_sent(arrived.at[0], x_send.at[0])
    all_sent(arrived.at[0, 0], s_send.at[0])
    all_sent(arrived.at[0:2, 1:groups], s_send.at[1])
    all_sent(edges, hal_send.at[0])
    all_sent(stats.at[0:3], stat_send.at[0])
    all_sent(swished.at[0:3], mix_send.at[0])
    all_sent(hidden.at[0:3], hid_send.at[0])
    all_sent(other_result, res_send.at[0])
    all_sent(summed.at[:, 1:groups], ret_send.at[0])


def pair_call(groups, parts, args):
    conv_value, expert_input, expert_gate, expert_down = args[0], args[2], args[3], args[5]
    out_weight, conv_kernel = args[6], args[7]
    channels, length = conv_value.shape
    count, model = expert_input.shape
    slots = count // groups
    quarter = model // parts
    units, wide = expert_gate.shape[2], expert_down.shape[2]
    out_width = out_weight.shape[1]
    edge = -(-((conv_kernel.shape[0] - 1) // 2) // 16) * 16
    cuts, pieces, blocks = 2, 2, groups // 2 + 1
    rows = groups * PAIR * slots
    piece = wide // pieces
    anywhere = pl.BlockSpec(memory_space=pl.ANY)
    near = pl.BlockSpec(memory_space=pltpu.VMEM)
    dma = pltpu.SemaphoreType.DMA
    return pl.pallas_call(
        functools.partial(pair_kernel, groups, parts),
        out_shape=(
            pltpu.VMEM((length, out_width), BF16),
            pltpu.VMEM((count, wide), BF16),
        ),
        in_specs=[anywhere] * 13,
        out_specs=(near, near),
        scratch_shapes=[
            pltpu.VMEM(args[7].shape, args[7].dtype),
            pltpu.VMEM((2, *args[8].shape), F32),
            *[pltpu.VMEM(arg.shape, arg.dtype) for arg in args[10:]],
            pltpu.VMEM((2, channels, length), BF16),
            pltpu.VMEM((count, quarter), BF16),
            pltpu.VMEM((count, model), BF16),
            pltpu.VMEM((2, model, units), BF16),
            pltpu.VMEM(expert_down.shape[1:], BF16),
            pltpu.VMEM(out_weight.shape, BF16),
            pltpu.VMEM((groups - 1, slots, quarter), BF16),
            pltpu.VMEM((groups, slots, 128), F32),
            pltpu.VMEM((groups, slots, 128), F32),
            pltpu.VMEM((parts, groups, PAIR, slots, quarter), BF16),
            pltpu.VMEM((rows, units), F32),
            pltpu.VMEM((rows, units), F32),
            pltpu.VMEM((parts, rows, units), BF16),
            pltpu.VMEM((rows, wide), F32),
            pltpu.VMEM((pieces, PAIR, groups, slots, piece), BF16),
            pltpu.VMEM((pieces, groups, slots, piece), BF16),
            pltpu.VMEM((pieces, groups, slots, piece), BF16),
            pltpu.VMEM((pieces, groups, slots, piece), BF16),
            pltpu.VMEM((count, groups * slots), BF16),
            pltpu.VMEM((length + 2 * edge, channels), F32),
            pltpu.VMEM((2, edge, channels), BF16),
            pltpu.VMEM((2, edge, channels), BF16),
            pltpu.VMEM((length, channels), BF16),
            pltpu.VMEM((parts, 2 * length // 128, 128), F32),
            pltpu.VMEM((parts, length, channels), BF16),
            dma((11,)),
            dma((1,)),
            dma((groups,)),
            dma((1,)),
            dma((1,)),
            dma((1,)),
            dma((groups,)),
            dma((1,)),
            dma((groups,)),
            dma((groups,)),
            dma((2,)),
            dma((blocks,)),
            dma((1,)),
            dma((1,)),
            dma((1,)),
            dma((1,)),
            dma((1,)),
            dma((2 * cuts + 1,)),
            dma((1,)),
            dma((3 * blocks,)),
            dma((1,)),
            dma((blocks * pieces,)),
            dma((1,)),
            dma((pieces,)),
        ],
        compiler_params=pltpu.CompilerParams(
            collective_id=0, has_side_effects=True, vmem_limit_bytes=60 * 1024 * 1024
        ),
        name="pair_block",
    )(*args)


def local(
    experts,
    parts,
    conv_value,
    conv_gate,
    conv_kernel,
    norm_gain,
    norm_shift,
    out_weight,
    expert_input,
    expert_ids,
    pair_logits,
    group_prob,
    expert_gate,
    expert_up,
    expert_down,
):
    channels, length = conv_value.shape
    count, model = expert_input.shape
    slots = 2 * count // experts
    rows = experts * slots
    half = model // CORES
    units, wide = expert_gate.shape[2], expert_down.shape[2]
    out_width = out_weight.shape[1]
    chips = parts // CORES
    args = (
        conv_value,
        conv_gate,
        expert_input,
        expert_gate,
        expert_up,
        expert_down,
        out_weight,
        conv_kernel,
        norm_gain[None, :],
        norm_shift[None, :],
        expert_ids.T,
        pair_logits.T,
        group_prob[None, :],
    )
    if experts == GROUPS * PAIR and chips == 2:
        return pair_call(GROUPS, parts, args)
    edge = -(-((conv_kernel.shape[0] - 1) // 2) // 16) * 16
    anywhere = pl.BlockSpec(memory_space=pl.ANY)
    near = pl.BlockSpec(memory_space=pltpu.VMEM)
    dma = pltpu.SemaphoreType.DMA
    return pl.pallas_call(
        functools.partial(kernel, experts, parts),
        out_shape=(
            pltpu.VMEM((length, out_width), BF16),
            pltpu.VMEM((count, wide), BF16),
        ),
        in_specs=[anywhere] * 7 + [near] * 6,
        out_specs=(anywhere, anywhere),
        scratch_shapes=[
            pltpu.VMEM((channels, length), BF16),
            pltpu.VMEM((channels, length), BF16),
            pltpu.VMEM((count, half), BF16),
            pltpu.VMEM((model, units), BF16),
            pltpu.VMEM((model, units), BF16),
            pltpu.VMEM(expert_down.shape[1:], BF16),
            pltpu.VMEM(out_weight.shape, BF16),
            pltpu.VMEM((experts, slots, half), BF16),
            pltpu.VMEM((CORES, experts, slots, half), BF16),
            pltpu.VMEM((rows, units), F32),
            pltpu.VMEM((rows, units), F32),
            pltpu.VMEM((parts, rows, units), BF16),
            pltpu.VMEM((rows, wide), F32),
            pltpu.VMEM((experts, slots, wide), BF16),
            pltpu.VMEM((experts, slots, wide), BF16),
            pltpu.VMEM((length + 2 * edge, channels), F32),
            pltpu.VMEM((2, edge, channels), BF16),
            pltpu.VMEM((2, edge, channels), BF16),
            pltpu.VMEM((parts, length, channels), BF16),
            pltpu.VMEM((parts, length, channels), BF16),
            pltpu.VMEM((length, out_width), BF16),
            pltpu.VMEM((count, wide), BF16),
            dma((7,)),
            dma((2,)),
            dma((2,)),
            dma((experts,)),
            dma((experts,)),
            dma((experts,)),
            dma((experts,)),
            dma((2,)),
            dma((2,)),
            dma((2 * chips,)),
            dma((2 * chips,)),
            dma((2 * chips,)),
            dma((2 * chips,)),
            dma((experts,)),
            dma((experts,)),
        ],
        compiler_params=pltpu.CompilerParams(
            collective_id=0, has_side_effects=True, vmem_limit_bytes=60 * 1024 * 1024
        ),
        name="block",
    )(*args)

def solution(mesh):
    placed = (
        P("tp", "ep"),
        P("tp", "ep"),
        P(None, "tp"),
        P(),
        P(),
        P(None, "tp"),
        P("ep", None),
        P("ep", None),
        P("ep", None),
        P("ep"),
        P("ep", None, "tp"),
        P("ep", None, "tp"),
        P("ep", None, "tp"),
    )
    return jax.shard_map(
        functools.partial(local, mesh.shape["ep"], mesh.shape["tp"]),
        mesh=mesh,
        in_specs=placed,
        out_specs=(P("ep", "tp"), P("ep", "tp")),
        check_vma=False,
    )
```

```python
import functools

import jax
import jax.numpy as jnp
from jax import lax
from jax.experimental import pallas as pl
from jax.experimental.pallas import tpu as pltpu
from jax.sharding import PartitionSpec as P

MESH = pl.DeviceIdType.MESH
CORES = 2
PAIR = 2
GROUPS = 4
F32, BF16 = jnp.float32, jnp.bfloat16


def tiles(size, most):
    tile = min(size, most)
    return tile, size // tile


def kernel(
    experts,
    parts,
    value_hbm,
    gate_hbm,
    input_hbm,
    wgate_hbm,
    wup_hbm,
    wdown_hbm,
    wout_hbm,
    taps_ref,
    gain_ref,
    shift_ref,
    ids_ref,
    logits_ref,
    prob_ref,
    mixer_hbm,
    expert_hbm,
    value,
    gate,
    tokens,
    wgate,
    wup,
    wdown,
    wout,
    send_rows,
    arrived,
    gate_sum,
    up_sum,
    hidden,
    down_sum,
    result,
    returned,
    padded,
    edges,
    halo,
    conv,
    swished,
    mixer,
    combined,
    load_sem,
    out_sem,
    self_sem,
    disp_send,
    disp_recv,
    fwd_send,
    fwd_recv,
    hal_send,
    hal_recv,
    conv_send,
    conv_recv,
    hid_send,
    hid_recv,
    ret_send,
    ret_recv,
):
    me = lax.axis_index("ep")
    tp = lax.axis_index("tp")
    chips = parts // CORES
    chip, core = lax.div(tp, CORES), lax.rem(tp, CORES)
    other = 1 - core
    sibling = chip * CORES + other
    slots = send_rows.shape[1]
    half = send_rows.shape[2]
    rows = experts * slots
    length, channels = conv.shape[1], conv.shape[2]
    edge = halo.shape[1]
    reach = (taps_ref.shape[0] - 1) // 2

    def remote(src, dst, ssem, rsem, ep=None, part=None):
        target = (me if ep is None else ep, tp if part is None else part)
        return pltpu.make_async_remote_copy(
            src_ref=src, dst_ref=dst, send_sem=ssem, recv_sem=rsem, device_id=target, device_id_type=MESH
        )

    def ahead(k):
        return lax.rem(me + k, experts)

    def behind(k):
        return lax.rem(me + experts - k, experts)

    def chip_ahead(k):
        return lax.rem(chip + k, chips) * CORES + core

    def chip_behind(k):
        return lax.rem(chip + chips - k, chips) * CORES + core

    barrier = pltpu.get_barrier_semaphore()

    @pl.loop(1, experts)
    def _(k):
        pl.semaphore_signal(barrier, inc=1, device_id=(ahead(k), tp), device_id_type=MESH)

    @pl.loop(1, chips)
    def _(k):
        pl.semaphore_signal(barrier, inc=1, device_id=(me, chip_ahead(k)), device_id_type=MESH)

    pl.semaphore_signal(barrier, inc=1, device_id=(me, sibling), device_id_type=MESH)

    columns = pl.ds(pl.multiple_of(core * half, half), half)
    loads = [
        pltpu.make_async_copy(src, dst, load_sem.at[i])
        for i, (src, dst) in enumerate(
            [
                (input_hbm.at[:, columns], tokens),
                (value_hbm, value),
                (gate_hbm, gate),
                (wgate_hbm.at[0], wgate),
                (wup_hbm.at[0], wup),
                (wout_hbm, wout),
                (wdown_hbm.at[0], wdown),
            ]
        )
    ]
    for load in loads:
        load.start()

    count = ids_ref.shape[1]
    first, second = ids_ref[0:1, :], ids_ref[1:2, :]
    expert_of = lax.broadcasted_iota(jnp.int32, (experts, count), 0)
    is_first, is_second = expert_of == first, expert_of == second
    chosen = jnp.where(is_first | is_second, 1.0, 0.0).astype(F32)
    earlier = lax.broadcasted_iota(jnp.int32, (count, count), 0) < lax.broadcasted_iota(
        jnp.int32, (count, count), 1
    )
    rank = jnp.dot(
        chosen.astype(BF16), jnp.where(earlier, 1.0, 0.0).astype(BF16), preferred_element_type=F32
    )
    rank = jnp.where(chosen > 0, rank, -1.0)
    ordinal = lax.broadcasted_iota(jnp.int32, (experts, slots, count), 1).astype(F32)
    place3 = jnp.broadcast_to(rank[:, None, :], (experts, slots, count)) == ordinal
    place = jnp.where(place3, 1.0, 0.0).astype(F32).reshape(rows, count)

    loads[0].wait()
    tile, steps = tiles(half, 512)
    for i in range(steps):
        span = slice(i * tile, (i + 1) * tile)
        picked = jnp.dot(place.astype(BF16), tokens[:, span], preferred_element_type=F32)
        send_rows[:, :, span] = picked.reshape(experts, slots, tile).astype(BF16)

    pl.semaphore_wait(barrier, experts - 1 + chips)

    def dispatch(k):
        return remote(
            send_rows.at[ahead(k)], arrived.at[core, me], disp_send.at[k], disp_recv.at[k], ep=ahead(k)
        )

    def forward(k, src):
        return remote(
            src, arrived.at[core, behind(k)], fwd_send.at[k], fwd_recv.at[k], part=sibling
        )

    @pl.loop(1, experts)
    def _(k):
        dispatch(k).start()

    keep = pltpu.make_async_copy(send_rows.at[me], arrived.at[core, me], self_sem.at[0])
    keep.start()
    forward(0, send_rows.at[me]).start()

    loads[1].wait()
    loads[2].wait()
    gated = (value[...].astype(F32) * jax.nn.sigmoid(gate[...].astype(F32))).astype(BF16)
    padded[edge : edge + length, :] = jnp.transpose(gated.astype(F32), (1, 0))
    edges[0] = padded[edge : 2 * edge, :].astype(BF16)
    edges[1] = padded[length : length + edge, :].astype(BF16)
    to_left = remote(edges.at[0], halo.at[1], hal_send.at[0], hal_recv.at[0], ep=behind(1))
    to_right = remote(edges.at[1], halo.at[0], hal_send.at[1], hal_recv.at[1], ep=ahead(1))
    to_left.start()
    to_right.start()
    taps = taps_ref[...].astype(F32)
    chunk, chunks = tiles(length, 64)

    def convolve(i):
        total = jnp.zeros((chunk, channels), F32)
        for j in range(taps.shape[0]):
            start = i * chunk + j + edge - reach
            total = total + taps[j : j + 1, :] * padded[start : start + chunk, :]
        conv[tp, i * chunk : (i + 1) * chunk, :] = total.astype(BF16)

    for i in range(1, chunks - 1):
        convolve(i)
    to_left.wait()
    to_right.wait()
    padded[0:edge, :] = jnp.where(me == 0, 0.0, halo[0].astype(F32))
    padded[edge + length : 2 * edge + length, :] = jnp.where(
        me == experts - 1, 0.0, halo[1].astype(F32)
    )
    convolve(0)
    convolve(chunks - 1)

    def gather(buffer, ssem, rsem):
        def across(k):
            return remote(buffer.at[tp], buffer.at[tp], ssem.at[k], rsem.at[k], part=chip_ahead(k))

        def beside(k):
            block = chip_behind(k)
            return remote(
                buffer.at[block], buffer.at[block], ssem.at[chips + k], rsem.at[chips + k], part=sibling
            )

        return across, beside

    conv_across, conv_beside = gather(conv, conv_send, conv_recv)

    @pl.loop(1, chips)
    def _(k):
        conv_across(k).start()

    conv_beside(0).start()

    @pl.loop(1, experts)
    def _(k):
        dispatch(k).wait_recv()
        forward(k, arrived.at[core, behind(k)]).start()

    keep.wait()
    loads[3].wait()
    loads[4].wait()
    units = gate_sum.shape[1]
    tile, steps = tiles(units, 256)

    def side(which):
        block = arrived[which]
        if slots % 16:
            return block.astype(F32).reshape(rows, half).astype(BF16)
        return block.reshape(rows, half)

    def depth(which):
        return pl.ds(pl.multiple_of(which * half, half), half)

    for i in range(steps):
        span = slice(i * tile, (i + 1) * tile)
        gate_sum[:, span] = jnp.dot(side(core), wgate[depth(core), span], preferred_element_type=F32)
        up_sum[:, span] = jnp.dot(side(core), wup[depth(core), span], preferred_element_type=F32)

    @pl.loop(0, experts)
    def _(k):
        forward(k, send_rows.at[me]).wait_recv()

    for i in range(steps):
        span = slice(i * tile, (i + 1) * tile)
        gate_val = gate_sum[:, span] + jnp.dot(
            side(other), wgate[depth(other), span], preferred_element_type=F32
        )
        up_val = up_sum[:, span] + jnp.dot(
            side(other), wup[depth(other), span], preferred_element_type=F32
        )
        hidden[tp, :, span] = (jax.nn.silu(gate_val) * up_val).astype(BF16)

    hid_across, hid_beside = gather(hidden, hid_send, hid_recv)

    @pl.loop(1, chips)
    def _(k):
        hid_across(k).start()

    hid_beside(0).start()

    @pl.loop(1, chips)
    def _(k):
        conv_across(k).wait_recv()
        conv_beside(k).start()

    @pl.loop(0, chips)
    def _(k):
        conv_beside(k).wait_recv()

    width = parts * channels
    chunk, chunks = tiles(length, 64)

    @pl.loop(0, chunks)
    def _(i):
        span = pl.ds(pl.multiple_of(i * chunk, chunk), chunk)
        blocks = [conv[b, span, :].astype(F32) for b in range(parts)]
        center = sum(jnp.sum(block, axis=1, keepdims=True) for block in blocks) / width
        blocks = [block - center for block in blocks]
        spread = sum(jnp.sum(block * block, axis=1, keepdims=True) for block in blocks) / width
        scale = lax.rsqrt(spread + 1e-05)
        for b in range(parts):
            lanes = slice(b * channels, (b + 1) * channels)
            normed = blocks[b] * scale * gain_ref[:, lanes] + shift_ref[:, lanes]
            swished[b, span, :] = jax.nn.silu(normed).astype(BF16)

    loads[6].wait()
    wide = down_sum.shape[1]
    tile, steps = tiles(wide, 256)

    def down(block, begin):
        deep = pl.ds(pl.multiple_of(block * units, units), units)

        @pl.loop(0, steps)
        def _(i):
            span = pl.ds(pl.multiple_of(i * tile, tile), tile)
            product = jnp.dot(hidden[block], wdown[deep, span], preferred_element_type=F32)
            down_sum[:, span] = product if begin else down_sum[:, span] + product

    down(tp, True)
    hid_beside(0).wait_recv()
    down(sibling, False)

    @pl.loop(1, chips)
    def _(k):
        hid_across(k).wait_recv()
        hid_beside(k).start()
        down(chip_behind(k), False)
        hid_beside(k).wait_recv()
        down(chip_behind(k) + other - core, False)

    result[...] = down_sum[...].reshape(experts, slots, wide).astype(BF16)

    def give_back(k):
        return remote(result.at[ahead(k)], returned.at[me], ret_send.at[k], ret_recv.at[k], ep=ahead(k))

    @pl.loop(1, experts)
    def _(k):
        give_back(k).start()

    own = pltpu.make_async_copy(result.at[me], returned.at[me], self_sem.at[1])
    own.start()

    loads[5].wait()
    tile, steps = tiles(mixer.shape[1], 256)

    @pl.loop(0, steps)
    def _(i):
        span = pl.ds(pl.multiple_of(i * tile, tile), tile)
        total = jnp.zeros((length, tile), F32)
        for b in range(parts):
            total = total + jnp.dot(
                swished[b], wout[b * channels : (b + 1) * channels, span], preferred_element_type=F32
            )
        mixer[:, span] = total.astype(BF16)

    put_mixer = pltpu.make_async_copy(mixer, mixer_hbm, out_sem.at[0])
    put_mixer.start()

    share = jax.nn.sigmoid(logits_ref[0:1, :] - logits_ref[1:2, :])
    weight = jnp.where(is_first, share * prob_ref[...], 0.0) + jnp.where(
        is_second, (1.0 - share) * prob_ref[...], 0.0
    )
    weights = jnp.where(
        place3, jnp.broadcast_to(weight[:, None, :], (experts, slots, count)), 0.0
    ).reshape(rows, count)
    weights = jnp.transpose(weights, (1, 0))
    high = weights.astype(BF16)
    rest = weights - high.astype(F32)
    middle = rest.astype(BF16)
    low = (rest - middle.astype(F32)).astype(BF16)

    own.wait()

    @pl.loop(1, experts)
    def _(k):
        give_back(k).wait_recv()

    tile, steps = tiles(wide, 512)
    for i in range(steps):
        span = slice(i * tile, (i + 1) * tile)
        block = returned[:, :, span]
        if slots % 16:
            block = block.astype(F32).reshape(rows, tile).astype(BF16)
        else:
            block = block.reshape(rows, tile)
        total = jnp.dot(low, block, preferred_element_type=F32)
        total = total + jnp.dot(middle, block, preferred_element_type=F32)
        total = total + jnp.dot(high, block, preferred_element_type=F32)
        combined[:, span] = total.astype(BF16)

    put_expert = pltpu.make_async_copy(combined, expert_hbm, out_sem.at[1])
    put_expert.start()

    @pl.loop(1, experts)
    def _(k):
        dispatch(k).wait_send()
        give_back(k).wait_send()

    @pl.loop(0, experts)
    def _(k):
        forward(k, send_rows.at[me]).wait_send()

    @pl.loop(1, chips)
    def _(k):
        conv_across(k).wait_send()
        hid_across(k).wait_send()

    @pl.loop(0, chips)
    def _(k):
        conv_beside(k).wait_send()
        hid_beside(k).wait_send()

    put_mixer.wait()
    put_expert.wait()


def pair_kernel(
    groups,
    parts,
    value_hbm,
    gate_hbm,
    input_hbm,
    wgate_hbm,
    wup_hbm,
    wdown_hbm,
    wout_hbm,
    taps_hbm,
    gain_hbm,
    shift_hbm,
    ids_hbm,
    logits_hbm,
    prob_hbm,
    mixer,
    returned,
    scatter,
    taps_ref,
    affine,
    ids_ref,
    logits_ref,
    prob_ref,
    values,
    mine,
    tokens,
    projections,
    wdown,
    wout,
    send_rows,
    weights,
    arrived_weights,
    arrived,
    gate_sum,
    up_sum,
    hidden,
    down_sum,
    result,
    other_result,
    summed,
    padded,
    edges,
    halo,
    conv,
    stats,
    swished,
    load_sem,
    z_send,
    z_recv,
    w_send,
    w_recv,
    y_send,
    y_recv,
    x_send,
    x_recv,
    d_recv,
    s_send,
    s_recv,
    hal_send,
    hal_recv,
    stat_send,
    stat_recv,
    mix_send,
    mix_recv,
    hid_send,
    hid_recv,
    res_send,
    res_recv,
    ret_send,
    ret_recv,
):
    experts = groups * PAIR
    me = lax.axis_index("ep")
    tp = lax.axis_index("tp")
    group, side = lax.div(me, PAIR), lax.rem(me, PAIR)
    mate = group * PAIR + 1 - side
    chip, core = lax.div(tp, CORES), lax.rem(tp, CORES)
    sibling = chip * CORES + 1 - core
    beside = (1 - chip) * CORES + core
    opposite = (1 - chip) * CORES + 1 - core
    slots, quarter = send_rows.shape[1], send_rows.shape[2]
    blocks = [(0, groups // 2)] + [(p, 1) for p in range(groups // 2, groups)]
    each = PAIR * slots
    straight = (1,)
    length, channels = conv.shape
    edge = halo.shape[1]
    reach = (taps_ref.shape[0] - 1) // 2

    def remote(src, dst, ssem, rsem, ep=None, part=None):
        target = (me if ep is None else ep, tp if part is None else part)
        return pltpu.make_async_remote_copy(
            src_ref=src, dst_ref=dst, send_sem=ssem, recv_sem=rsem, device_id=target, device_id_type=MESH
        )

    def onward(k):
        return jnp.bitwise_xor(group, k) * PAIR + side

    def backward(k):
        return jnp.bitwise_xor(group, k) * PAIR + side

    left, right = lax.rem(me + experts - 1, experts), lax.rem(me + 1, experts)
    barrier = pltpu.get_barrier_semaphore()
    peers = [(onward(k), tp) for k in range(1, groups)]
    peers += [(mate, tp), (me, beside), (me, sibling), (me, opposite), (mate, beside), (left, tp), (right, tp)]
    for peer in peers:
        pl.semaphore_signal(barrier, inc=1, device_id=peer, device_id_type=MESH)

    columns = pl.ds(pl.multiple_of(tp * quarter, quarter), quarter)
    def load(i, *pairs):
        return [pltpu.make_async_copy(src, dst, load_sem.at[i]) for src, dst in pairs]

    loads = [
        load(0, (ids_hbm, ids_ref)),
        load(1, (input_hbm.at[:, columns], mine)),
        load(2, (logits_hbm, logits_ref)),
        load(3, (prob_hbm, prob_ref)),
        load(4, (input_hbm, tokens)),
        load(5, (value_hbm, values.at[0]), (gate_hbm, values.at[1])),
        load(6, (taps_hbm, taps_ref)),
        load(7, (wgate_hbm, projections.at[0:1]), (wup_hbm, projections.at[1:2])),
        load(8, (wdown_hbm.at[0], wdown)),
        load(9, (wout_hbm, wout)),
        load(10, (gain_hbm, affine.at[0]), (shift_hbm, affine.at[1])),
    ]
    for copies in loads:
        for copy in copies:
            copy.start()

    def loaded(i):
        whole = {5: values, 7: projections, 10: affine}.get(i)
        if whole is None:
            loads[i][0].wait()
        else:
            pltpu.make_async_copy(whole, whole, load_sem.at[i]).wait()

    loaded(0)

    count = ids_ref.shape[1]
    first, second = ids_ref[0:1, :], ids_ref[1:2, :]
    position = jnp.bitwise_xor(lax.broadcasted_iota(jnp.int32, (groups, count), 0), group) * PAIR
    chosen = jnp.where((first >= position) & (first < position + PAIR), 1.0, 0.0).astype(F32)
    earlier = lax.broadcasted_iota(jnp.int32, (count, count), 0) < lax.broadcasted_iota(
        jnp.int32, (count, count), 1
    )
    rank = jnp.dot(
        chosen.astype(BF16), jnp.where(earlier, 1.0, 0.0).astype(BF16), preferred_element_type=F32
    )
    rank = jnp.where(chosen > 0, rank, -1.0)
    ordinal = lax.broadcasted_iota(jnp.int32, (groups, slots, count), 1).astype(F32)
    place3 = jnp.broadcast_to(rank[:, None, :], (groups, slots, count)) == ordinal
    place_f = jnp.where(place3, 1.0, 0.0).astype(F32).reshape(groups * slots, count)
    place = place_f.astype(BF16)

    def dispatch(k):
        return remote(
            send_rows.at[k - 1],
            arrived.at[tp, k, 0],
            z_send.at[0],
            z_recv.at[k],
            ep=onward(k),
        )

    loaded(1)
    picked = jnp.dot(place[slots:], mine[...], preferred_element_type=F32)
    send_rows[...] = picked.astype(BF16).reshape(groups - 1, slots, quarter)
    pl.semaphore_wait(barrier, len(peers))
    for k in range(1, groups):
        dispatch(k).start()

    def to_beside(p):
        return remote(
            arrived.at[tp, p, 0], arrived.at[tp, p, 0], y_send.at[0], y_recv.at[p], part=beside
        )

    def to_mate(p):
        return remote(arrived.at[tp, p, 0], arrived.at[tp, p, 1], x_send.at[0], x_recv.at[p], ep=mate)

    def across(p):
        if p == 0:
            return remote(
                arrived.at[beside, 0, 0], arrived.at[beside, 0, 1], x_send.at[0], d_recv.at[0], ep=mate
            )
        if p in straight:
            return remote(
                arrived.at[tp, p, 0], arrived.at[tp, p, 1], x_send.at[0], d_recv.at[p], ep=mate, part=beside
            )
        return remote(
            arrived.at[beside, p, 0], arrived.at[beside, p, 1], x_send.at[0], d_recv.at[p], ep=mate
        )

    def to_sibling(p, far, which):
        block = beside if far else tp
        return remote(
            arrived.at[block, p, which],
            arrived.at[block, p, which],
            s_send.at[min(p, 1)],
            s_recv.at[sum(start <= p for start, _ in blocks) - 1],
            part=sibling,
        )

    def all_sent(whole, sem):
        remote(whole, whole, sem, sem, part=sibling).wait_send()

    def all_received(whole, sem):
        remote(whole, whole, sem, sem, part=sibling).wait_recv()

    loaded(4)
    for q in range(parts):
        picked = jnp.dot(
            place[:slots], tokens[:, q * quarter : (q + 1) * quarter], preferred_element_type=F32
        )
        arrived[q, 0, 0] = picked.astype(BF16)
    to_mate(0).start()
    across(0).start()

    loaded(2)
    loaded(3)
    share = jax.nn.sigmoid(logits_ref[0:1, :] - logits_ref[1:2, :])
    of_first = share * prob_ref[...]
    of_second = (1.0 - share) * prob_ref[...]
    first_mine = (first < second) == (side == 0)
    own_weight = jnp.sum(place_f * jnp.where(first_mine, of_first, of_second), axis=1, keepdims=True)
    mate_weight = jnp.sum(place_f * jnp.where(first_mine, of_second, of_first), axis=1, keepdims=True)
    lane = lax.broadcasted_iota(jnp.int32, (groups * slots, weights.shape[2]), 1)
    both = jnp.where(lane < weights.shape[2] // 2, own_weight, mate_weight)
    weights[...] = both.reshape(weights.shape)

    def give_weights(k):
        return remote(weights.at[k], arrived_weights.at[k], w_send.at[0], w_recv.at[0], ep=onward(k))

    arrived_weights[0] = weights[0]
    scatter[...] = jnp.transpose(place_f, (1, 0)).astype(BF16)

    loaded(5)
    loaded(6)
    gated = (values[0].astype(F32) * jax.nn.sigmoid(values[1].astype(F32))).astype(BF16)
    padded[edge : edge + length, :] = jnp.transpose(gated.astype(F32), (1, 0))
    edges[0] = padded[edge : 2 * edge, :].astype(BF16)
    edges[1] = padded[length : length + edge, :].astype(BF16)
    to_left = remote(edges.at[0], halo.at[1], hal_send.at[0], hal_recv.at[0], ep=left)
    to_right = remote(edges.at[1], halo.at[0], hal_send.at[0], hal_recv.at[0], ep=right)
    to_left.start()
    to_right.start()
    for k in range(1, groups):
        give_weights(k).start()
    taps = taps_ref[...].astype(F32)
    chunk, chunks = tiles(length, 64)

    def convolve(i):
        total = jnp.zeros((chunk, channels), F32)
        for j in range(taps.shape[0]):
            start = i * chunk + j + edge - reach
            total = total + taps[j : j + 1, :] * padded[start : start + chunk, :]
        conv[i * chunk : (i + 1) * chunk, :] = total.astype(BF16)

    def landed(p):
        dispatch(p).wait_recv()
        to_beside(p).start()
        to_mate(p).start()
        if p in straight:
            across(p).start()
        to_sibling(p, 0, 0).start()

    def turned(p):
        to_beside(p).wait_recv()
        if p not in straight:
            across(p).start()
        to_sibling(p, 1, 0).start()

    def met(p):
        to_mate(p).wait_recv()
        to_sibling(p, 0, 1).start()

    def closed(p):
        across(p).wait_recv()
        to_sibling(p, 1, 1).start()

    def measure():
        block = conv[...].astype(F32)
        center = jnp.sum(block, axis=1, keepdims=True) / channels
        block = block - center
        spread = jnp.sum(block * block, axis=1, keepdims=True)
        lane = lax.broadcasted_iota(jnp.int32, (length, 128), 1)
        turned_over = jnp.transpose(jnp.where(lane == 0, center, spread), (1, 0))
        lanes = stats.shape[2]
        for i in range(length // lanes):
            span = slice(i * lanes, (i + 1) * lanes)
            stats[tp, i : i + 1] = turned_over[0:1, span]
            stats[tp, i + length // lanes : i + 1 + length // lanes] = turned_over[1:2, span]
        for i in range(3):
            tell(i).start()

    def tell(i):
        part = (sibling, beside, opposite)[i]
        return remote(stats.at[tp], stats.at[tp], stat_send.at[0], stat_recv.at[0], part=part)

    def normalize():
        all_received(stats.at[0:3], stat_recv.at[0])
        wraps = length // stats.shape[2]
        centers = [stats[b, 0:wraps] for b in range(parts)]
        center = sum(centers) / parts
        spread = sum(
            stats[b, wraps : 2 * wraps] + channels * jnp.square(centers[b] - center) for b in range(parts)
        )
        scale = lax.rsqrt(spread / (parts * channels) + 1e-05)
        row = lax.broadcasted_iota(jnp.int32, (128, stats.shape[2]), 0)
        turned_over = [
            jnp.transpose(jnp.where(row == 0, center[i : i + 1], scale[i : i + 1]), (1, 0)) for i in range(wraps)
        ]
        across_rows = jnp.concatenate(turned_over, axis=0)
        center, scale = across_rows[:, 0:1], across_rows[:, 1:2]
        lanes = pl.ds(pl.multiple_of(tp * channels, channels), channels)
        normed = (conv[...].astype(F32) - center) * scale * affine[0, :, lanes] + affine[1, :, lanes]
        swished[tp] = jax.nn.silu(normed).astype(BF16)

    cuts = mix_recv.shape[0] // 2
    share_rows = length // cuts

    def share_copy(i, kind):
        cut = pl.ds(i * share_rows, share_rows)
        block = beside if kind == 2 else tp
        j = 2 * cuts if kind == 1 else 2 * i + kind // 2
        return remote(
            swished.at[block, cut],
            swished.at[block, cut],
            mix_send.at[0],
            mix_recv.at[j],
            part=beside if kind == 0 else sibling,
        )

    units = hidden.shape[2]
    tile, steps = tiles(units, 256)

    def extent(h):
        start, size = blocks[h]
        return slice(start * each, (start + size) * each)

    def deep(q):
        return pl.ds(pl.multiple_of(q * quarter, quarter), quarter)

    def project(h, quarters, begin):
        start, size = blocks[h]
        for i in range(steps):
            span = slice(i * tile, (i + 1) * tile)
            for which, total in enumerate((gate_sum, up_sum)):
                product = sum(
                    jnp.dot(
                        arrived[q, start : start + size].reshape(size * each, quarter),
                        projections[which, deep(q), span],
                        preferred_element_type=F32,
                    )
                    for q in quarters
                )
                total[extent(h), span] = product if begin else total[extent(h), span] + product

    def hid_copy(h, kind):
        block = beside if kind == 2 else tp
        j = 3 * h + kind
        return remote(
            hidden.at[block, extent(h)],
            hidden.at[block, extent(h)],
            hid_send.at[0],
            hid_recv.at[j],
            part=beside if kind == 0 else sibling,
        )

    def near(h):
        project(h, (tp,), True)

    def next_near(h):
        project(h, (beside,), False)

    def far(h):
        start, size = blocks[h]
        whole = arrived.at[0:2, start : start + size] if start else arrived.at[0 : 2 * size - 1, 0]
        all_received(whole, s_recv.at[h])
        project(h, (sibling, opposite), False)
        hidden[tp, extent(h)] = (jax.nn.silu(gate_sum[extent(h)]) * up_sum[extent(h)]).astype(BF16)
        hid_copy(h, 0).start()
        hid_copy(h, 1).start()

    wide = down_sum.shape[1]
    pieces = result.shape[0]
    span_wide = wide // pieces
    cols = [slice(c * span_wide, (c + 1) * span_wide) for c in range(pieces)]

    def down(h, block, c):
        depth = pl.ds(pl.multiple_of(block * units, units), units)
        return jnp.dot(hidden[block, extent(h)], wdown[depth, cols[c]], preferred_element_type=F32)

    def down_near(h):
        hid_copy(h, 1).wait_recv()
        for c in range(pieces):
            down_sum[extent(h), cols[c]] = down(h, tp, c) + down(h, sibling, c)

    def hand_on(h):
        hid_copy(h, 0).wait_recv()
        hid_copy(h, 2).start()

    def exchange(p, c):
        return remote(
            result.at[c, 1, p],
            other_result.at[c, p],
            res_send.at[0],
            res_recv.at[pieces * p + c],
            ep=mate,
        )

    def down_far(h):
        start, size = blocks[h]
        for c in range(pieces):
            down_sum[extent(h), cols[c]] += down(h, beside, c)
        hid_copy(h, 2).wait_recv()
        for c in range(pieces):
            total = (down_sum[extent(h), cols[c]] + down(h, opposite, c)).astype(BF16)
            total = total.reshape(size, PAIR, slots, span_wide)
            for which in range(PAIR):
                result[c, which, start : start + size] = total[:, which]
            for p in range(max(start, 1), start + size):
                exchange(p, c).start()

    def give_back(k, c):
        return remote(summed.at[c, k], returned.at[c, k], ret_send.at[0], ret_recv.at[c], ep=backward(k))

    def combine(k):
        middle = weights.shape[2] // 2
        ours = arrived_weights[k, :, 0:1]
        theirs = arrived_weights[k, :, middle : middle + 1]
        for c in range(pieces):
            exchange(k, c).wait_recv()
            total = ours * result[c, 0, k].astype(F32) + theirs * other_result[c, k].astype(F32)
            if k:
                summed[c, k] = total.astype(BF16)
                give_back(k, c).start()
            else:
                returned[c, 0] = total.astype(BF16)

    out_tile, out_steps = tiles(mixer.shape[1], 256)

    def mix(cut):
        cut_rows = pl.ds(cut * share_rows, share_rows)

        for i in range(out_steps):
            span = slice(i * out_tile, (i + 1) * out_tile)
            total = sum(
                jnp.dot(swished[b, cut_rows], wout[b * channels : (b + 1) * channels, span], preferred_element_type=F32)
                for b in range(parts)
            )
            mixer[cut_rows, span] = total.astype(BF16)

    def passed(i):
        share_copy(i, 0).wait_recv()
        share_copy(i, 2).start()

    def mixed(i):
        if i == 0:
            all_received(swished.at[0], mix_recv.at[2 * cuts])
        share_copy(i, 2).wait_recv()
        mix(i)

    for i in range(1, chunks - 1):
        convolve(i)
    landed(1)
    met(0)
    closed(0)
    landed(2)
    landed(3)
    turned(1)
    met(1)
    loaded(7)
    near(0)
    all_received(halo, hal_recv.at[0])
    padded[0:edge, :] = jnp.where(me == 0, 0.0, halo[0].astype(F32))
    padded[edge + length : 2 * edge + length, :] = jnp.where(
        me == experts - 1, 0.0, halo[1].astype(F32)
    )
    convolve(0)
    convolve(chunks - 1)
    measure()
    closed(1)
    next_near(0)
    turned(2)
    far(0)
    turned(3)
    met(2)
    near(1)
    met(3)
    near(2)
    loaded(8)
    down_near(0)
    loaded(10)
    normalize()
    for i in range(cuts):
        share_copy(i, 1).start()
    closed(2)
    next_near(1)
    far(1)
    closed(3)
    next_near(2)
    hand_on(0)
    far(2)
    for i in range(cuts):
        share_copy(i, 0).start()
    down_far(0)
    down_near(1)
    hand_on(1)
    down_near(2)
    down_far(1)
    hand_on(2)
    all_received(arrived_weights.at[1:groups], w_recv.at[0])
    down_far(2)
    for c in range(pieces):
        exchange(0, c).start()
    combine(1)
    combine(2)
    passed(0)
    combine(3)
    loaded(9)
    mixed(0)
    combine(0)
    for i in range(1, cuts):
        passed(i)
        mixed(i)
    for c in range(pieces):
        all_received(returned.at[c, 1:groups], ret_recv.at[c])
    all_sent(send_rows, z_send.at[0])
    all_sent(weights.at[1:groups], w_send.at[0])
    all_sent(arrived.at[0, 1:groups, 0], y_send.at[0])
    all_sent(arrived.at[0], x_send.at[0])
    all_sent(arrived.at[0, 0], s_send.at[0])
    all_sent(arrived.at[0:2, 1:groups], s_send.at[1])
    all_sent(edges, hal_send.at[0])
    all_sent(stats.at[0:3], stat_send.at[0])
    all_sent(swished.at[0:3], mix_send.at[0])
    all_sent(hidden.at[0:3], hid_send.at[0])
    all_sent(other_result, res_send.at[0])
    all_sent(summed.at[:, 1:groups], ret_send.at[0])


def store(mixer, returned, scatter, mixer_hbm, combined_hbm, combined, sem):
    put_mixer = pltpu.make_async_copy(mixer, mixer_hbm, sem.at[0])
    put_mixer.start()
    pieces, groups, slots, piece = returned.shape
    for c in range(pieces):
        combined[:, c * piece : (c + 1) * piece] = jnp.dot(
            scatter[...], returned[c].reshape(groups * slots, piece), preferred_element_type=F32
        ).astype(BF16)
    put_combined = pltpu.make_async_copy(combined, combined_hbm, sem.at[1])
    put_combined.start()
    put_mixer.wait()
    put_combined.wait()


def pair_call(groups, parts, args):
    conv_value, expert_input, expert_gate, expert_down = args[0], args[2], args[3], args[5]
    out_weight, conv_kernel = args[6], args[7]
    channels, length = conv_value.shape
    count, model = expert_input.shape
    slots = count // groups
    quarter = model // parts
    units, wide = expert_gate.shape[2], expert_down.shape[2]
    out_width = out_weight.shape[1]
    edge = -(-((conv_kernel.shape[0] - 1) // 2) // 16) * 16
    cuts, pieces, blocks = 2, 2, groups // 2 + 1
    rows = groups * PAIR * slots
    piece = wide // pieces
    anywhere = pl.BlockSpec(memory_space=pl.ANY)
    near = pl.BlockSpec(memory_space=pltpu.VMEM)
    dma = pltpu.SemaphoreType.DMA
    results = pl.pallas_call(
        functools.partial(pair_kernel, groups, parts),
        out_shape=(
            pltpu.VMEM((length, out_width), BF16),
            pltpu.VMEM((pieces, groups, slots, piece), BF16),
            pltpu.VMEM((count, groups * slots), BF16),
        ),
        in_specs=[anywhere] * 13,
        out_specs=(near, near, near),
        scratch_shapes=[
            pltpu.VMEM(args[7].shape, args[7].dtype),
            pltpu.VMEM((2, *args[8].shape), F32),
            *[pltpu.VMEM(arg.shape, arg.dtype) for arg in args[10:]],
            pltpu.VMEM((2, channels, length), BF16),
            pltpu.VMEM((count, quarter), BF16),
            pltpu.VMEM((count, model), BF16),
            pltpu.VMEM((2, model, units), BF16),
            pltpu.VMEM(expert_down.shape[1:], BF16),
            pltpu.VMEM(out_weight.shape, BF16),
            pltpu.VMEM((groups - 1, slots, quarter), BF16),
            pltpu.VMEM((groups, slots, 128), F32),
            pltpu.VMEM((groups, slots, 128), F32),
            pltpu.VMEM((parts, groups, PAIR, slots, quarter), BF16),
            pltpu.VMEM((rows, units), F32),
            pltpu.VMEM((rows, units), F32),
            pltpu.VMEM((parts, rows, units), BF16),
            pltpu.VMEM((rows, wide), F32),
            pltpu.VMEM((pieces, PAIR, groups, slots, piece), BF16),
            pltpu.VMEM((pieces, groups, slots, piece), BF16),
            pltpu.VMEM((pieces, groups, slots, piece), BF16),
            pltpu.VMEM((length + 2 * edge, channels), F32),
            pltpu.VMEM((2, edge, channels), BF16),
            pltpu.VMEM((2, edge, channels), BF16),
            pltpu.VMEM((length, channels), BF16),
            pltpu.VMEM((parts, 2 * length // 128, 128), F32),
            pltpu.VMEM((parts, length, channels), BF16),
            dma((11,)),
            dma((1,)),
            dma((groups,)),
            dma((1,)),
            dma((1,)),
            dma((1,)),
            dma((groups,)),
            dma((1,)),
            dma((groups,)),
            dma((groups,)),
            dma((2,)),
            dma((blocks,)),
            dma((1,)),
            dma((1,)),
            dma((1,)),
            dma((1,)),
            dma((1,)),
            dma((2 * cuts + 1,)),
            dma((1,)),
            dma((3 * blocks,)),
            dma((1,)),
            dma((groups * pieces,)),
            dma((1,)),
            dma((pieces,)),
        ],
        compiler_params=pltpu.CompilerParams(
            collective_id=0, has_side_effects=True, vmem_limit_bytes=60 * 1024 * 1024
        ),
        name="pair_block",
    )(*args)
    results = [pltpu.with_memory_space_constraint(value, pltpu.VMEM) for value in results]
    return pl.pallas_call(
        store,
        out_shape=(
            jax.ShapeDtypeStruct((length, out_width), BF16),
            jax.ShapeDtypeStruct((count, wide), BF16),
        ),
        in_specs=[near] * 3,
        out_specs=(pl.BlockSpec(memory_space=pltpu.HBM),) * 2,
        scratch_shapes=[pltpu.VMEM((count, wide), BF16), dma((2,))],
        name="store",
    )(*results)


def local(
    experts,
    parts,
    conv_value,
    conv_gate,
    conv_kernel,
    norm_gain,
    norm_shift,
    out_weight,
    expert_input,
    expert_ids,
    pair_logits,
    group_prob,
    expert_gate,
    expert_up,
    expert_down,
):
    channels, length = conv_value.shape
    count, model = expert_input.shape
    slots = 2 * count // experts
    rows = experts * slots
    half = model // CORES
    units, wide = expert_gate.shape[2], expert_down.shape[2]
    out_width = out_weight.shape[1]
    chips = parts // CORES
    args = (
        conv_value,
        conv_gate,
        expert_input,
        expert_gate,
        expert_up,
        expert_down,
        out_weight,
        conv_kernel,
        norm_gain[None, :],
        norm_shift[None, :],
        expert_ids.T,
        pair_logits.T,
        group_prob[None, :],
    )
    if experts == GROUPS * PAIR and chips == 2:
        return pair_call(GROUPS, parts, args)
    edge = -(-((conv_kernel.shape[0] - 1) // 2) // 16) * 16
    anywhere = pl.BlockSpec(memory_space=pl.ANY)
    near = pl.BlockSpec(memory_space=pltpu.VMEM)
    dma = pltpu.SemaphoreType.DMA
    return pl.pallas_call(
        functools.partial(kernel, experts, parts),
        out_shape=(
            pltpu.VMEM((length, out_width), BF16),
            pltpu.VMEM((count, wide), BF16),
        ),
        in_specs=[anywhere] * 7 + [near] * 6,
        out_specs=(anywhere, anywhere),
        scratch_shapes=[
            pltpu.VMEM((channels, length), BF16),
            pltpu.VMEM((channels, length), BF16),
            pltpu.VMEM((count, half), BF16),
            pltpu.VMEM((model, units), BF16),
            pltpu.VMEM((model, units), BF16),
            pltpu.VMEM(expert_down.shape[1:], BF16),
            pltpu.VMEM(out_weight.shape, BF16),
            pltpu.VMEM((experts, slots, half), BF16),
            pltpu.VMEM((CORES, experts, slots, half), BF16),
            pltpu.VMEM((rows, units), F32),
            pltpu.VMEM((rows, units), F32),
            pltpu.VMEM((parts, rows, units), BF16),
            pltpu.VMEM((rows, wide), F32),
            pltpu.VMEM((experts, slots, wide), BF16),
            pltpu.VMEM((experts, slots, wide), BF16),
            pltpu.VMEM((length + 2 * edge, channels), F32),
            pltpu.VMEM((2, edge, channels), BF16),
            pltpu.VMEM((2, edge, channels), BF16),
            pltpu.VMEM((parts, length, channels), BF16),
            pltpu.VMEM((parts, length, channels), BF16),
            pltpu.VMEM((length, out_width), BF16),
            pltpu.VMEM((count, wide), BF16),
            dma((7,)),
            dma((2,)),
            dma((2,)),
            dma((experts,)),
            dma((experts,)),
            dma((experts,)),
            dma((experts,)),
            dma((2,)),
            dma((2,)),
            dma((2 * chips,)),
            dma((2 * chips,)),
            dma((2 * chips,)),
            dma((2 * chips,)),
            dma((experts,)),
            dma((experts,)),
        ],
        compiler_params=pltpu.CompilerParams(
            collective_id=0, has_side_effects=True, vmem_limit_bytes=60 * 1024 * 1024
        ),
        name="block",
    )(*args)

def solution(mesh):
    placed = (
        P("tp", "ep"),
        P("tp", "ep"),
        P(None, "tp"),
        P(),
        P(),
        P(None, "tp"),
        P("ep", None),
        P("ep", None),
        P("ep", None),
        P("ep"),
        P("ep", None, "tp"),
        P("ep", None, "tp"),
        P("ep", None, "tp"),
    )
    return jax.shard_map(
        functools.partial(local, mesh.shape["ep"], mesh.shape["tp"]),
        mesh=mesh,
        in_specs=placed,
        out_specs=(P("ep", "tp"), P("ep", "tp")),
        check_vma=False,
    )
```

```python
import functools

import jax
import jax.numpy as jnp
from jax import lax
from jax.experimental import pallas as pl
from jax.experimental.pallas import tpu as pltpu
from jax.sharding import PartitionSpec as P

MESH = pl.DeviceIdType.MESH
CORES = 2
PAIR = 2
GROUPS = 4
F32, BF16 = jnp.float32, jnp.bfloat16


def tiles(size, most):
    tile = min(size, most)
    return tile, size // tile


def kernel(
    experts,
    parts,
    value_hbm,
    gate_hbm,
    input_hbm,
    wgate_hbm,
    wup_hbm,
    wdown_hbm,
    wout_hbm,
    taps_ref,
    gain_ref,
    shift_ref,
    ids_ref,
    logits_ref,
    prob_ref,
    mixer_hbm,
    expert_hbm,
    value,
    gate,
    tokens,
    wgate,
    wup,
    wdown,
    wout,
    send_rows,
    arrived,
    gate_sum,
    up_sum,
    hidden,
    down_sum,
    result,
    returned,
    padded,
    edges,
    halo,
    conv,
    swished,
    mixer,
    combined,
    load_sem,
    out_sem,
    self_sem,
    disp_send,
    disp_recv,
    fwd_send,
    fwd_recv,
    hal_send,
    hal_recv,
    conv_send,
    conv_recv,
    hid_send,
    hid_recv,
    ret_send,
    ret_recv,
):
    me = lax.axis_index("ep")
    tp = lax.axis_index("tp")
    chips = parts // CORES
    chip, core = lax.div(tp, CORES), lax.rem(tp, CORES)
    other = 1 - core
    sibling = chip * CORES + other
    slots = send_rows.shape[1]
    half = send_rows.shape[2]
    rows = experts * slots
    length, channels = conv.shape[1], conv.shape[2]
    edge = halo.shape[1]
    reach = (taps_ref.shape[0] - 1) // 2

    def remote(src, dst, ssem, rsem, ep=None, part=None):
        target = (me if ep is None else ep, tp if part is None else part)
        return pltpu.make_async_remote_copy(
            src_ref=src, dst_ref=dst, send_sem=ssem, recv_sem=rsem, device_id=target, device_id_type=MESH
        )

    def ahead(k):
        return lax.rem(me + k, experts)

    def behind(k):
        return lax.rem(me + experts - k, experts)

    def chip_ahead(k):
        return lax.rem(chip + k, chips) * CORES + core

    def chip_behind(k):
        return lax.rem(chip + chips - k, chips) * CORES + core

    barrier = pltpu.get_barrier_semaphore()

    @pl.loop(1, experts)
    def _(k):
        pl.semaphore_signal(barrier, inc=1, device_id=(ahead(k), tp), device_id_type=MESH)

    @pl.loop(1, chips)
    def _(k):
        pl.semaphore_signal(barrier, inc=1, device_id=(me, chip_ahead(k)), device_id_type=MESH)

    pl.semaphore_signal(barrier, inc=1, device_id=(me, sibling), device_id_type=MESH)

    columns = pl.ds(pl.multiple_of(core * half, half), half)
    loads = [
        pltpu.make_async_copy(src, dst, load_sem.at[i])
        for i, (src, dst) in enumerate(
            [
                (input_hbm.at[:, columns], tokens),
                (value_hbm, value),
                (gate_hbm, gate),
                (wgate_hbm.at[0], wgate),
                (wup_hbm.at[0], wup),
                (wout_hbm, wout),
                (wdown_hbm.at[0], wdown),
            ]
        )
    ]
    for load in loads:
        load.start()

    count = ids_ref.shape[1]
    first, second = ids_ref[0:1, :], ids_ref[1:2, :]
    expert_of = lax.broadcasted_iota(jnp.int32, (experts, count), 0)
    is_first, is_second = expert_of == first, expert_of == second
    chosen = jnp.where(is_first | is_second, 1.0, 0.0).astype(F32)
    earlier = lax.broadcasted_iota(jnp.int32, (count, count), 0) < lax.broadcasted_iota(
        jnp.int32, (count, count), 1
    )
    rank = jnp.dot(
        chosen.astype(BF16), jnp.where(earlier, 1.0, 0.0).astype(BF16), preferred_element_type=F32
    )
    rank = jnp.where(chosen > 0, rank, -1.0)
    ordinal = lax.broadcasted_iota(jnp.int32, (experts, slots, count), 1).astype(F32)
    place3 = jnp.broadcast_to(rank[:, None, :], (experts, slots, count)) == ordinal
    place = jnp.where(place3, 1.0, 0.0).astype(F32).reshape(rows, count)

    loads[0].wait()
    tile, steps = tiles(half, 512)
    for i in range(steps):
        span = slice(i * tile, (i + 1) * tile)
        picked = jnp.dot(place.astype(BF16), tokens[:, span], preferred_element_type=F32)
        send_rows[:, :, span] = picked.reshape(experts, slots, tile).astype(BF16)

    pl.semaphore_wait(barrier, experts - 1 + chips)

    def dispatch(k):
        return remote(
            send_rows.at[ahead(k)], arrived.at[core, me], disp_send.at[k], disp_recv.at[k], ep=ahead(k)
        )

    def forward(k, src):
        return remote(
            src, arrived.at[core, behind(k)], fwd_send.at[k], fwd_recv.at[k], part=sibling
        )

    @pl.loop(1, experts)
    def _(k):
        dispatch(k).start()

    keep = pltpu.make_async_copy(send_rows.at[me], arrived.at[core, me], self_sem.at[0])
    keep.start()
    forward(0, send_rows.at[me]).start()

    loads[1].wait()
    loads[2].wait()
    gated = (value[...].astype(F32) * jax.nn.sigmoid(gate[...].astype(F32))).astype(BF16)
    padded[edge : edge + length, :] = jnp.transpose(gated.astype(F32), (1, 0))
    edges[0] = padded[edge : 2 * edge, :].astype(BF16)
    edges[1] = padded[length : length + edge, :].astype(BF16)
    to_left = remote(edges.at[0], halo.at[1], hal_send.at[0], hal_recv.at[0], ep=behind(1))
    to_right = remote(edges.at[1], halo.at[0], hal_send.at[1], hal_recv.at[1], ep=ahead(1))
    to_left.start()
    to_right.start()
    taps = taps_ref[...].astype(F32)
    chunk, chunks = tiles(length, 64)

    def convolve(i):
        total = jnp.zeros((chunk, channels), F32)
        for j in range(taps.shape[0]):
            start = i * chunk + j + edge - reach
            total = total + taps[j : j + 1, :] * padded[start : start + chunk, :]
        conv[tp, i * chunk : (i + 1) * chunk, :] = total.astype(BF16)

    for i in range(1, chunks - 1):
        convolve(i)
    to_left.wait()
    to_right.wait()
    padded[0:edge, :] = jnp.where(me == 0, 0.0, halo[0].astype(F32))
    padded[edge + length : 2 * edge + length, :] = jnp.where(
        me == experts - 1, 0.0, halo[1].astype(F32)
    )
    convolve(0)
    convolve(chunks - 1)

    def gather(buffer, ssem, rsem):
        def across(k):
            return remote(buffer.at[tp], buffer.at[tp], ssem.at[k], rsem.at[k], part=chip_ahead(k))

        def beside(k):
            block = chip_behind(k)
            return remote(
                buffer.at[block], buffer.at[block], ssem.at[chips + k], rsem.at[chips + k], part=sibling
            )

        return across, beside

    conv_across, conv_beside = gather(conv, conv_send, conv_recv)

    @pl.loop(1, chips)
    def _(k):
        conv_across(k).start()

    conv_beside(0).start()

    @pl.loop(1, experts)
    def _(k):
        dispatch(k).wait_recv()
        forward(k, arrived.at[core, behind(k)]).start()

    keep.wait()
    loads[3].wait()
    loads[4].wait()
    units = gate_sum.shape[1]
    tile, steps = tiles(units, 256)

    def side(which):
        block = arrived[which]
        if slots % 16:
            return block.astype(F32).reshape(rows, half).astype(BF16)
        return block.reshape(rows, half)

    def depth(which):
        return pl.ds(pl.multiple_of(which * half, half), half)

    for i in range(steps):
        span = slice(i * tile, (i + 1) * tile)
        gate_sum[:, span] = jnp.dot(side(core), wgate[depth(core), span], preferred_element_type=F32)
        up_sum[:, span] = jnp.dot(side(core), wup[depth(core), span], preferred_element_type=F32)

    @pl.loop(0, experts)
    def _(k):
        forward(k, send_rows.at[me]).wait_recv()

    for i in range(steps):
        span = slice(i * tile, (i + 1) * tile)
        gate_val = gate_sum[:, span] + jnp.dot(
            side(other), wgate[depth(other), span], preferred_element_type=F32
        )
        up_val = up_sum[:, span] + jnp.dot(
            side(other), wup[depth(other), span], preferred_element_type=F32
        )
        hidden[tp, :, span] = (jax.nn.silu(gate_val) * up_val).astype(BF16)

    hid_across, hid_beside = gather(hidden, hid_send, hid_recv)

    @pl.loop(1, chips)
    def _(k):
        hid_across(k).start()

    hid_beside(0).start()

    @pl.loop(1, chips)
    def _(k):
        conv_across(k).wait_recv()
        conv_beside(k).start()

    @pl.loop(0, chips)
    def _(k):
        conv_beside(k).wait_recv()

    width = parts * channels
    chunk, chunks = tiles(length, 64)

    @pl.loop(0, chunks)
    def _(i):
        span = pl.ds(pl.multiple_of(i * chunk, chunk), chunk)
        blocks = [conv[b, span, :].astype(F32) for b in range(parts)]
        center = sum(jnp.sum(block, axis=1, keepdims=True) for block in blocks) / width
        blocks = [block - center for block in blocks]
        spread = sum(jnp.sum(block * block, axis=1, keepdims=True) for block in blocks) / width
        scale = lax.rsqrt(spread + 1e-05)
        for b in range(parts):
            lanes = slice(b * channels, (b + 1) * channels)
            normed = blocks[b] * scale * gain_ref[:, lanes] + shift_ref[:, lanes]
            swished[b, span, :] = jax.nn.silu(normed).astype(BF16)

    loads[6].wait()
    wide = down_sum.shape[1]
    tile, steps = tiles(wide, 256)

    def down(block, begin):
        deep = pl.ds(pl.multiple_of(block * units, units), units)

        @pl.loop(0, steps)
        def _(i):
            span = pl.ds(pl.multiple_of(i * tile, tile), tile)
            product = jnp.dot(hidden[block], wdown[deep, span], preferred_element_type=F32)
            down_sum[:, span] = product if begin else down_sum[:, span] + product

    down(tp, True)
    hid_beside(0).wait_recv()
    down(sibling, False)

    @pl.loop(1, chips)
    def _(k):
        hid_across(k).wait_recv()
        hid_beside(k).start()
        down(chip_behind(k), False)
        hid_beside(k).wait_recv()
        down(chip_behind(k) + other - core, False)

    result[...] = down_sum[...].reshape(experts, slots, wide).astype(BF16)

    def give_back(k):
        return remote(result.at[ahead(k)], returned.at[me], ret_send.at[k], ret_recv.at[k], ep=ahead(k))

    @pl.loop(1, experts)
    def _(k):
        give_back(k).start()

    own = pltpu.make_async_copy(result.at[me], returned.at[me], self_sem.at[1])
    own.start()

    loads[5].wait()
    tile, steps = tiles(mixer.shape[1], 256)

    @pl.loop(0, steps)
    def _(i):
        span = pl.ds(pl.multiple_of(i * tile, tile), tile)
        total = jnp.zeros((length, tile), F32)
        for b in range(parts):
            total = total + jnp.dot(
                swished[b], wout[b * channels : (b + 1) * channels, span], preferred_element_type=F32
            )
        mixer[:, span] = total.astype(BF16)

    put_mixer = pltpu.make_async_copy(mixer, mixer_hbm, out_sem.at[0])
    put_mixer.start()

    share = jax.nn.sigmoid(logits_ref[0:1, :] - logits_ref[1:2, :])
    weight = jnp.where(is_first, share * prob_ref[...], 0.0) + jnp.where(
        is_second, (1.0 - share) * prob_ref[...], 0.0
    )
    weights = jnp.where(
        place3, jnp.broadcast_to(weight[:, None, :], (experts, slots, count)), 0.0
    ).reshape(rows, count)
    weights = jnp.transpose(weights, (1, 0))
    high = weights.astype(BF16)
    rest = weights - high.astype(F32)
    middle = rest.astype(BF16)
    low = (rest - middle.astype(F32)).astype(BF16)

    own.wait()

    @pl.loop(1, experts)
    def _(k):
        give_back(k).wait_recv()

    tile, steps = tiles(wide, 512)
    for i in range(steps):
        span = slice(i * tile, (i + 1) * tile)
        block = returned[:, :, span]
        if slots % 16:
            block = block.astype(F32).reshape(rows, tile).astype(BF16)
        else:
            block = block.reshape(rows, tile)
        total = jnp.dot(low, block, preferred_element_type=F32)
        total = total + jnp.dot(middle, block, preferred_element_type=F32)
        total = total + jnp.dot(high, block, preferred_element_type=F32)
        combined[:, span] = total.astype(BF16)

    put_expert = pltpu.make_async_copy(combined, expert_hbm, out_sem.at[1])
    put_expert.start()

    @pl.loop(1, experts)
    def _(k):
        dispatch(k).wait_send()
        give_back(k).wait_send()

    @pl.loop(0, experts)
    def _(k):
        forward(k, send_rows.at[me]).wait_send()

    @pl.loop(1, chips)
    def _(k):
        conv_across(k).wait_send()
        hid_across(k).wait_send()

    @pl.loop(0, chips)
    def _(k):
        conv_beside(k).wait_send()
        hid_beside(k).wait_send()

    put_mixer.wait()
    put_expert.wait()


def pair_kernel(
    groups,
    parts,
    value_hbm,
    gate_hbm,
    input_hbm,
    wgate_hbm,
    wup_hbm,
    wdown_hbm,
    wout_hbm,
    taps_hbm,
    gain_hbm,
    shift_hbm,
    ids_hbm,
    logits_hbm,
    prob_hbm,
    mixer,
    returned,
    scatter,
    taps_ref,
    affine,
    ids_ref,
    logits_ref,
    prob_ref,
    values,
    mine,
    tokens,
    projections,
    wdown,
    wout,
    send_rows,
    weights,
    arrived_weights,
    arrived,
    gate_sum,
    up_sum,
    hidden,
    down_sum,
    result,
    other_result,
    summed,
    padded,
    edges,
    halo,
    conv,
    stats,
    swished,
    load_sem,
    z_send,
    z_recv,
    w_send,
    w_recv,
    y_send,
    y_recv,
    x_send,
    x_recv,
    d_recv,
    s_send,
    s_recv,
    hal_send,
    hal_recv,
    stat_send,
    stat_recv,
    mix_send,
    mix_recv,
    hid_send,
    hid_recv,
    res_send,
    res_recv,
    ret_send,
    ret_recv,
):
    experts = groups * PAIR
    me = lax.axis_index("ep")
    tp = lax.axis_index("tp")
    group, side = lax.div(me, PAIR), lax.rem(me, PAIR)
    mate = group * PAIR + 1 - side
    chip, core = lax.div(tp, CORES), lax.rem(tp, CORES)
    sibling = chip * CORES + 1 - core
    beside = (1 - chip) * CORES + core
    opposite = (1 - chip) * CORES + 1 - core
    slots, quarter = send_rows.shape[1], send_rows.shape[2]
    blocks = [(0, groups // 2)] + [(p, 1) for p in range(groups // 2, groups)]
    each = PAIR * slots
    straight = (1,)
    length, channels = conv.shape
    edge = halo.shape[1]
    reach = (taps_ref.shape[0] - 1) // 2

    def remote(src, dst, ssem, rsem, ep=None, part=None):
        target = (me if ep is None else ep, tp if part is None else part)
        return pltpu.make_async_remote_copy(
            src_ref=src, dst_ref=dst, send_sem=ssem, recv_sem=rsem, device_id=target, device_id_type=MESH
        )

    def onward(k):
        return jnp.bitwise_xor(group, k) * PAIR + side

    def backward(k):
        return jnp.bitwise_xor(group, k) * PAIR + side

    left, right = lax.rem(me + experts - 1, experts), lax.rem(me + 1, experts)
    barrier = pltpu.get_barrier_semaphore()
    peers = [(onward(k), tp) for k in range(1, groups)]
    peers += [(mate, tp), (me, beside), (me, sibling), (me, opposite), (mate, beside), (left, tp), (right, tp)]
    for peer in peers:
        pl.semaphore_signal(barrier, inc=1, device_id=peer, device_id_type=MESH)

    columns = pl.ds(pl.multiple_of(tp * quarter, quarter), quarter)
    def load(i, *pairs):
        return [pltpu.make_async_copy(src, dst, load_sem.at[i]) for src, dst in pairs]

    loads = [
        load(0, (ids_hbm, ids_ref)),
        load(1, (input_hbm.at[:, columns], mine)),
        load(2, (logits_hbm, logits_ref)),
        load(3, (prob_hbm, prob_ref)),
        load(4, (input_hbm, tokens)),
        load(5, (value_hbm, values.at[0]), (gate_hbm, values.at[1])),
        load(6, (taps_hbm, taps_ref)),
        load(7, (wgate_hbm, projections.at[0:1]), (wup_hbm, projections.at[1:2])),
        load(8, (wdown_hbm.at[0], wdown)),
        load(9, (wout_hbm, wout)),
        load(10, (gain_hbm, affine.at[0]), (shift_hbm, affine.at[1])),
    ]
    for copies in loads:
        for copy in copies:
            copy.start()

    def loaded(i):
        whole = {5: values, 7: projections, 10: affine}.get(i)
        if whole is None:
            loads[i][0].wait()
        else:
            pltpu.make_async_copy(whole, whole, load_sem.at[i]).wait()

    loaded(0)

    count = ids_ref.shape[1]
    first, second = ids_ref[0:1, :], ids_ref[1:2, :]
    position = jnp.bitwise_xor(lax.broadcasted_iota(jnp.int32, (groups, count), 0), group) * PAIR
    chosen = jnp.where((first >= position) & (first < position + PAIR), 1.0, 0.0).astype(F32)
    earlier = lax.broadcasted_iota(jnp.int32, (count, count), 0) < lax.broadcasted_iota(
        jnp.int32, (count, count), 1
    )
    rank = jnp.dot(
        chosen.astype(BF16), jnp.where(earlier, 1.0, 0.0).astype(BF16), preferred_element_type=F32
    )
    rank = jnp.where(chosen > 0, rank, -1.0)
    ordinal = lax.broadcasted_iota(jnp.int32, (groups, slots, count), 1).astype(F32)
    place3 = jnp.broadcast_to(rank[:, None, :], (groups, slots, count)) == ordinal
    place_f = jnp.where(place3, 1.0, 0.0).astype(F32).reshape(groups * slots, count)
    place = place_f.astype(BF16)

    def dispatch(k):
        return remote(
            send_rows.at[k - 1],
            arrived.at[tp, k, 0],
            z_send.at[0],
            z_recv.at[k],
            ep=onward(k),
        )

    loaded(1)
    picked = jnp.dot(place[slots:], mine[...], preferred_element_type=F32)
    send_rows[...] = picked.astype(BF16).reshape(groups - 1, slots, quarter)
    pl.semaphore_wait(barrier, len(peers))
    for k in range(1, groups):
        dispatch(k).start()

    def to_beside(p):
        return remote(
            arrived.at[tp, p, 0], arrived.at[tp, p, 0], y_send.at[0], y_recv.at[p], part=beside
        )

    def to_mate(p):
        return remote(arrived.at[tp, p, 0], arrived.at[tp, p, 1], x_send.at[0], x_recv.at[p], ep=mate)

    def across(p):
        if p == 0:
            return remote(
                arrived.at[beside, 0, 0], arrived.at[beside, 0, 1], x_send.at[0], d_recv.at[0], ep=mate
            )
        if p in straight:
            return remote(
                arrived.at[tp, p, 0], arrived.at[tp, p, 1], x_send.at[0], d_recv.at[p], ep=mate, part=beside
            )
        return remote(
            arrived.at[beside, p, 0], arrived.at[beside, p, 1], x_send.at[0], d_recv.at[p], ep=mate
        )

    def to_sibling(p, far, which):
        block = beside if far else tp
        return remote(
            arrived.at[block, p, which],
            arrived.at[block, p, which],
            s_send.at[min(p, 1)],
            s_recv.at[2 * sum(start <= p for start, _ in blocks) - 2 + far],
            part=sibling,
        )

    def all_sent(whole, sem):
        remote(whole, whole, sem, sem, part=sibling).wait_send()

    def all_received(whole, sem):
        remote(whole, whole, sem, sem, part=sibling).wait_recv()

    loaded(4)
    for q in range(parts):
        picked = jnp.dot(
            place[:slots], tokens[:, q * quarter : (q + 1) * quarter], preferred_element_type=F32
        )
        arrived[q, 0, 0] = picked.astype(BF16)
    to_mate(0).start()
    across(0).start()

    loaded(2)
    loaded(3)
    share = jax.nn.sigmoid(logits_ref[0:1, :] - logits_ref[1:2, :])
    of_first = share * prob_ref[...]
    of_second = (1.0 - share) * prob_ref[...]
    first_mine = (first < second) == (side == 0)
    own_weight = jnp.sum(place_f * jnp.where(first_mine, of_first, of_second), axis=1, keepdims=True)
    mate_weight = jnp.sum(place_f * jnp.where(first_mine, of_second, of_first), axis=1, keepdims=True)
    lane = lax.broadcasted_iota(jnp.int32, (groups * slots, weights.shape[2]), 1)
    both = jnp.where(lane < weights.shape[2] // 2, own_weight, mate_weight)
    weights[...] = both.reshape(weights.shape)

    def give_weights(k):
        return remote(weights.at[k], arrived_weights.at[k], w_send.at[0], w_recv.at[0], ep=onward(k))

    arrived_weights[0] = weights[0]
    scatter[...] = jnp.transpose(place_f, (1, 0)).astype(BF16)

    loaded(5)
    loaded(6)
    gated = (values[0].astype(F32) * jax.nn.sigmoid(values[1].astype(F32))).astype(BF16)
    padded[edge : edge + length, :] = jnp.transpose(gated.astype(F32), (1, 0))
    edges[0] = padded[edge : 2 * edge, :].astype(BF16)
    edges[1] = padded[length : length + edge, :].astype(BF16)
    to_left = remote(edges.at[0], halo.at[1], hal_send.at[0], hal_recv.at[0], ep=left)
    to_right = remote(edges.at[1], halo.at[0], hal_send.at[0], hal_recv.at[0], ep=right)
    to_left.start()
    to_right.start()
    for k in range(1, groups):
        give_weights(k).start()
    taps = taps_ref[...].astype(F32)
    chunk, chunks = tiles(length, 64)

    def convolve(i):
        total = jnp.zeros((chunk, channels), F32)
        for j in range(taps.shape[0]):
            start = i * chunk + j + edge - reach
            total = total + taps[j : j + 1, :] * padded[start : start + chunk, :]
        conv[i * chunk : (i + 1) * chunk, :] = total.astype(BF16)

    def landed(p):
        dispatch(p).wait_recv()
        to_beside(p).start()
        to_mate(p).start()
        if p in straight:
            across(p).start()
        to_sibling(p, 0, 0).start()

    def turned(p):
        to_beside(p).wait_recv()
        if p not in straight:
            across(p).start()
        to_sibling(p, 1, 0).start()

    def met(p):
        to_mate(p).wait_recv()
        to_sibling(p, 0, 1).start()

    def closed(p):
        across(p).wait_recv()
        to_sibling(p, 1, 1).start()

    def measure():
        block = conv[...].astype(F32)
        center = jnp.sum(block, axis=1, keepdims=True) / channels
        block = block - center
        spread = jnp.sum(block * block, axis=1, keepdims=True)
        lane = lax.broadcasted_iota(jnp.int32, (length, 128), 1)
        turned_over = jnp.transpose(jnp.where(lane == 0, center, spread), (1, 0))
        lanes = stats.shape[2]
        for i in range(length // lanes):
            span = slice(i * lanes, (i + 1) * lanes)
            stats[tp, i : i + 1] = turned_over[0:1, span]
            stats[tp, i + length // lanes : i + 1 + length // lanes] = turned_over[1:2, span]
        for i in range(3):
            tell(i).start()

    def tell(i):
        part = (sibling, beside, opposite)[i]
        return remote(stats.at[tp], stats.at[tp], stat_send.at[0], stat_recv.at[0], part=part)

    def normalize():
        all_received(stats.at[0:3], stat_recv.at[0])
        wraps = length // stats.shape[2]
        centers = [stats[b, 0:wraps] for b in range(parts)]
        center = sum(centers) / parts
        spread = sum(
            stats[b, wraps : 2 * wraps] + channels * jnp.square(centers[b] - center) for b in range(parts)
        )
        scale = lax.rsqrt(spread / (parts * channels) + 1e-05)
        row = lax.broadcasted_iota(jnp.int32, (128, stats.shape[2]), 0)
        turned_over = [
            jnp.transpose(jnp.where(row == 0, center[i : i + 1], scale[i : i + 1]), (1, 0)) for i in range(wraps)
        ]
        across_rows = jnp.concatenate(turned_over, axis=0)
        center, scale = across_rows[:, 0:1], across_rows[:, 1:2]
        lanes = pl.ds(pl.multiple_of(tp * channels, channels), channels)
        normed = (conv[...].astype(F32) - center) * scale * affine[0, :, lanes] + affine[1, :, lanes]
        swished[tp] = jax.nn.silu(normed).astype(BF16)

    cuts = mix_recv.shape[0] // 2
    share_rows = length // cuts

    def share_copy(i, kind):
        cut = pl.ds(i * share_rows, share_rows)
        block = beside if kind == 2 else tp
        j = 2 * cuts if kind == 1 else 2 * i + kind // 2
        return remote(
            swished.at[block, cut],
            swished.at[block, cut],
            mix_send.at[0],
            mix_recv.at[j],
            part=beside if kind == 0 else sibling,
        )

    units = hidden.shape[2]
    tile, steps = tiles(units, 256)

    def extent(h):
        start, size = blocks[h]
        return slice(start * each, (start + size) * each)

    def deep(q):
        return pl.ds(pl.multiple_of(q * quarter, quarter), quarter)

    def project(h, quarters, begin):
        start, size = blocks[h]
        for i in range(steps):
            span = slice(i * tile, (i + 1) * tile)
            for which, total in enumerate((gate_sum, up_sum)):
                product = sum(
                    jnp.dot(
                        arrived[q, start : start + size].reshape(size * each, quarter),
                        projections[which, deep(q), span],
                        preferred_element_type=F32,
                    )
                    for q in quarters
                )
                total[extent(h), span] = product if begin else total[extent(h), span] + product

    def hid_copy(h, kind):
        block = beside if kind == 2 else tp
        j = 3 * h + kind
        return remote(
            hidden.at[block, extent(h)],
            hidden.at[block, extent(h)],
            hid_send.at[0],
            hid_recv.at[j],
            part=beside if kind == 0 else sibling,
        )

    def near(h):
        project(h, (tp,), True)

    def next_near(h):
        project(h, (beside,), False)

    def from_sibling(h, beyond):
        start, size = blocks[h]
        whole = arrived.at[0, start : start + size] if start else arrived.at[0 : 2 * size - 1, 0, 0]
        all_received(whole, s_recv.at[2 * h + beyond])
        project(h, (opposite if beyond else sibling,), False)

    def activate(h):
        hidden[tp, extent(h)] = (jax.nn.silu(gate_sum[extent(h)]) * up_sum[extent(h)]).astype(BF16)
        hid_copy(h, 0).start()
        hid_copy(h, 1).start()

    def finish(h):
        from_sibling(h, 1)
        activate(h)

    wide = down_sum.shape[1]
    pieces = result.shape[0]
    span_wide = wide // pieces
    cols = [slice(c * span_wide, (c + 1) * span_wide) for c in range(pieces)]

    def down(h, block, c):
        depth = pl.ds(pl.multiple_of(block * units, units), units)
        return jnp.dot(hidden[block, extent(h)], wdown[depth, cols[c]], preferred_element_type=F32)

    def down_near(h):
        hid_copy(h, 1).wait_recv()
        for c in range(pieces):
            down_sum[extent(h), cols[c]] = down(h, tp, c) + down(h, sibling, c)

    def hand_on(h):
        hid_copy(h, 0).wait_recv()
        hid_copy(h, 2).start()

    def exchange(p, c):
        return remote(
            result.at[c, 1, p],
            other_result.at[c, p],
            res_send.at[0],
            res_recv.at[pieces * p + c],
            ep=mate,
        )

    def down_far(h):
        start, size = blocks[h]
        for c in range(pieces):
            down_sum[extent(h), cols[c]] += down(h, beside, c)
        hid_copy(h, 2).wait_recv()
        for c in range(pieces):
            total = (down_sum[extent(h), cols[c]] + down(h, opposite, c)).astype(BF16)
            total = total.reshape(size, PAIR, slots, span_wide)
            for which in range(PAIR):
                result[c, which, start : start + size] = total[:, which]
            for p in range(max(start, 1), start + size):
                exchange(p, c).start()

    def give_back(k, c):
        return remote(summed.at[c, k], returned.at[c, k], ret_send.at[0], ret_recv.at[c], ep=backward(k))

    def combine(k):
        middle = weights.shape[2] // 2
        ours = arrived_weights[k, :, 0:1]
        theirs = arrived_weights[k, :, middle : middle + 1]
        for c in range(pieces):
            exchange(k, c).wait_recv()
            total = ours * result[c, 0, k].astype(F32) + theirs * other_result[c, k].astype(F32)
            if k:
                summed[c, k] = total.astype(BF16)
                give_back(k, c).start()
            else:
                returned[c, 0] = total.astype(BF16)

    out_tile, out_steps = tiles(mixer.shape[1], 256)

    def mix(cut):
        cut_rows = pl.ds(cut * share_rows, share_rows)

        for i in range(out_steps):
            span = slice(i * out_tile, (i + 1) * out_tile)
            total = sum(
                jnp.dot(swished[b, cut_rows], wout[b * channels : (b + 1) * channels, span], preferred_element_type=F32)
                for b in range(parts)
            )
            mixer[cut_rows, span] = total.astype(BF16)

    def passed(i):
        share_copy(i, 0).wait_recv()
        share_copy(i, 2).start()

    def mixed(i):
        if i == 0:
            all_received(swished.at[0], mix_recv.at[2 * cuts])
        share_copy(i, 2).wait_recv()
        mix(i)

    for i in range(1, chunks - 1):
        convolve(i)
    landed(1)
    met(0)
    closed(0)
    landed(2)
    landed(3)
    turned(1)
    met(1)
    loaded(7)
    near(0)
    all_received(halo, hal_recv.at[0])
    padded[0:edge, :] = jnp.where(me == 0, 0.0, halo[0].astype(F32))
    padded[edge + length : 2 * edge + length, :] = jnp.where(
        me == experts - 1, 0.0, halo[1].astype(F32)
    )
    convolve(0)
    convolve(chunks - 1)
    measure()
    closed(1)
    next_near(0)
    turned(2)
    from_sibling(0, 0)
    finish(0)
    turned(3)
    met(2)
    near(1)
    met(3)
    near(2)
    from_sibling(1, 0)
    from_sibling(2, 0)
    loaded(8)
    down_near(0)
    closed(2)
    next_near(1)
    loaded(10)
    normalize()
    finish(1)
    closed(3)
    next_near(2)
    hand_on(0)
    finish(2)
    for kind in (1, 0):
        for i in range(cuts):
            share_copy(i, kind).start()
    down_far(0)
    down_near(1)
    hand_on(1)
    down_near(2)
    down_far(1)
    hand_on(2)
    all_received(arrived_weights.at[1:groups], w_recv.at[0])
    down_far(2)
    for c in range(pieces):
        exchange(0, c).start()
    combine(1)
    combine(2)
    combine(3)
    passed(0)
    combine(0)
    loaded(9)
    mixed(0)
    for i in range(1, cuts):
        passed(i)
        mixed(i)
    for c in range(pieces):
        all_received(returned.at[c, 1:groups], ret_recv.at[c])
    all_sent(send_rows, z_send.at[0])
    all_sent(weights.at[1:groups], w_send.at[0])
    all_sent(arrived.at[0, 1:groups, 0], y_send.at[0])
    all_sent(arrived.at[0], x_send.at[0])
    all_sent(arrived.at[0, 0], s_send.at[0])
    all_sent(arrived.at[0:2, 1:groups], s_send.at[1])
    all_sent(edges, hal_send.at[0])
    all_sent(stats.at[0:3], stat_send.at[0])
    all_sent(swished.at[0:3], mix_send.at[0])
    all_sent(hidden.at[0:3], hid_send.at[0])
    all_sent(other_result, res_send.at[0])
    all_sent(summed.at[:, 1:groups], ret_send.at[0])


def store(mixer, returned, scatter, mixer_hbm, combined_hbm, combined, sem):
    put_mixer = pltpu.make_async_copy(mixer, mixer_hbm, sem.at[0])
    put_mixer.start()
    pieces, groups, slots, piece = returned.shape
    for c in range(pieces):
        combined[:, c * piece : (c + 1) * piece] = jnp.dot(
            scatter[...], returned[c].reshape(groups * slots, piece), preferred_element_type=F32
        ).astype(BF16)
    put_combined = pltpu.make_async_copy(combined, combined_hbm, sem.at[1])
    put_combined.start()
    put_mixer.wait()
    put_combined.wait()


def pair_call(groups, parts, args):
    conv_value, expert_input, expert_gate, expert_down = args[0], args[2], args[3], args[5]
    out_weight, conv_kernel = args[6], args[7]
    channels, length = conv_value.shape
    count, model = expert_input.shape
    slots = count // groups
    quarter = model // parts
    units, wide = expert_gate.shape[2], expert_down.shape[2]
    out_width = out_weight.shape[1]
    edge = -(-((conv_kernel.shape[0] - 1) // 2) // 16) * 16
    cuts, pieces, blocks = 2, 2, groups // 2 + 1
    rows = groups * PAIR * slots
    piece = wide // pieces
    anywhere = pl.BlockSpec(memory_space=pl.ANY)
    near = pl.BlockSpec(memory_space=pltpu.VMEM)
    dma = pltpu.SemaphoreType.DMA
    results = pl.pallas_call(
        functools.partial(pair_kernel, groups, parts),
        out_shape=(
            pltpu.VMEM((length, out_width), BF16),
            pltpu.VMEM((pieces, groups, slots, piece), BF16),
            pltpu.VMEM((count, groups * slots), BF16),
        ),
        in_specs=[anywhere] * 13,
        out_specs=(near, near, near),
        scratch_shapes=[
            pltpu.VMEM(args[7].shape, args[7].dtype),
            pltpu.VMEM((2, *args[8].shape), F32),
            *[pltpu.VMEM(arg.shape, arg.dtype) for arg in args[10:]],
            pltpu.VMEM((2, channels, length), BF16),
            pltpu.VMEM((count, quarter), BF16),
            pltpu.VMEM((count, model), BF16),
            pltpu.VMEM((2, model, units), BF16),
            pltpu.VMEM(expert_down.shape[1:], BF16),
            pltpu.VMEM(out_weight.shape, BF16),
            pltpu.VMEM((groups - 1, slots, quarter), BF16),
            pltpu.VMEM((groups, slots, 128), F32),
            pltpu.VMEM((groups, slots, 128), F32),
            pltpu.VMEM((parts, groups, PAIR, slots, quarter), BF16),
            pltpu.VMEM((rows, units), F32),
            pltpu.VMEM((rows, units), F32),
            pltpu.VMEM((parts, rows, units), BF16),
            pltpu.VMEM((rows, wide), F32),
            pltpu.VMEM((pieces, PAIR, groups, slots, piece), BF16),
            pltpu.VMEM((pieces, groups, slots, piece), BF16),
            pltpu.VMEM((pieces, groups, slots, piece), BF16),
            pltpu.VMEM((length + 2 * edge, channels), F32),
            pltpu.VMEM((2, edge, channels), BF16),
            pltpu.VMEM((2, edge, channels), BF16),
            pltpu.VMEM((length, channels), BF16),
            pltpu.VMEM((parts, 2 * length // 128, 128), F32),
            pltpu.VMEM((parts, length, channels), BF16),
            dma((11,)),
            dma((1,)),
            dma((groups,)),
            dma((1,)),
            dma((1,)),
            dma((1,)),
            dma((groups,)),
            dma((1,)),
            dma((groups,)),
            dma((groups,)),
            dma((2,)),
            dma((2 * blocks,)),
            dma((1,)),
            dma((1,)),
            dma((1,)),
            dma((1,)),
            dma((1,)),
            dma((2 * cuts + 1,)),
            dma((1,)),
            dma((3 * blocks,)),
            dma((1,)),
            dma((groups * pieces,)),
            dma((1,)),
            dma((pieces,)),
        ],
        compiler_params=pltpu.CompilerParams(
            collective_id=0, has_side_effects=True, vmem_limit_bytes=60 * 1024 * 1024
        ),
        name="pair_block",
    )(*args)
    results = [pltpu.with_memory_space_constraint(value, pltpu.VMEM) for value in results]
    return pl.pallas_call(
        store,
        out_shape=(
            jax.ShapeDtypeStruct((length, out_width), BF16),
            jax.ShapeDtypeStruct((count, wide), BF16),
        ),
        in_specs=[near] * 3,
        out_specs=(pl.BlockSpec(memory_space=pltpu.HBM),) * 2,
        scratch_shapes=[pltpu.VMEM((count, wide), BF16), dma((2,))],
        name="store",
    )(*results)


def local(
    experts,
    parts,
    conv_value,
    conv_gate,
    conv_kernel,
    norm_gain,
    norm_shift,
    out_weight,
    expert_input,
    expert_ids,
    pair_logits,
    group_prob,
    expert_gate,
    expert_up,
    expert_down,
):
    channels, length = conv_value.shape
    count, model = expert_input.shape
    slots = 2 * count // experts
    rows = experts * slots
    half = model // CORES
    units, wide = expert_gate.shape[2], expert_down.shape[2]
    out_width = out_weight.shape[1]
    chips = parts // CORES
    args = (
        conv_value,
        conv_gate,
        expert_input,
        expert_gate,
        expert_up,
        expert_down,
        out_weight,
        conv_kernel,
        norm_gain[None, :],
        norm_shift[None, :],
        expert_ids.T,
        pair_logits.T,
        group_prob[None, :],
    )
    if experts == GROUPS * PAIR and chips == 2:
        return pair_call(GROUPS, parts, args)
    edge = -(-((conv_kernel.shape[0] - 1) // 2) // 16) * 16
    anywhere = pl.BlockSpec(memory_space=pl.ANY)
    near = pl.BlockSpec(memory_space=pltpu.VMEM)
    dma = pltpu.SemaphoreType.DMA
    return pl.pallas_call(
        functools.partial(kernel, experts, parts),
        out_shape=(
            pltpu.VMEM((length, out_width), BF16),
            pltpu.VMEM((count, wide), BF16),
        ),
        in_specs=[anywhere] * 7 + [near] * 6,
        out_specs=(anywhere, anywhere),
        scratch_shapes=[
            pltpu.VMEM((channels, length), BF16),
            pltpu.VMEM((channels, length), BF16),
            pltpu.VMEM((count, half), BF16),
            pltpu.VMEM((model, units), BF16),
            pltpu.VMEM((model, units), BF16),
            pltpu.VMEM(expert_down.shape[1:], BF16),
            pltpu.VMEM(out_weight.shape, BF16),
            pltpu.VMEM((experts, slots, half), BF16),
            pltpu.VMEM((CORES, experts, slots, half), BF16),
            pltpu.VMEM((rows, units), F32),
            pltpu.VMEM((rows, units), F32),
            pltpu.VMEM((parts, rows, units), BF16),
            pltpu.VMEM((rows, wide), F32),
            pltpu.VMEM((experts, slots, wide), BF16),
            pltpu.VMEM((experts, slots, wide), BF16),
            pltpu.VMEM((length + 2 * edge, channels), F32),
            pltpu.VMEM((2, edge, channels), BF16),
            pltpu.VMEM((2, edge, channels), BF16),
            pltpu.VMEM((parts, length, channels), BF16),
            pltpu.VMEM((parts, length, channels), BF16),
            pltpu.VMEM((length, out_width), BF16),
            pltpu.VMEM((count, wide), BF16),
            dma((7,)),
            dma((2,)),
            dma((2,)),
            dma((experts,)),
            dma((experts,)),
            dma((experts,)),
            dma((experts,)),
            dma((2,)),
            dma((2,)),
            dma((2 * chips,)),
            dma((2 * chips,)),
            dma((2 * chips,)),
            dma((2 * chips,)),
            dma((experts,)),
            dma((experts,)),
        ],
        compiler_params=pltpu.CompilerParams(
            collective_id=0, has_side_effects=True, vmem_limit_bytes=60 * 1024 * 1024
        ),
        name="block",
    )(*args)

def solution(mesh):
    placed = (
        P("tp", "ep"),
        P("tp", "ep"),
        P(None, "tp"),
        P(),
        P(),
        P(None, "tp"),
        P("ep", None),
        P("ep", None),
        P("ep", None),
        P("ep"),
        P("ep", None, "tp"),
        P("ep", None, "tp"),
        P("ep", None, "tp"),
    )
    return jax.shard_map(
        functools.partial(local, mesh.shape["ep"], mesh.shape["tp"]),
        mesh=mesh,
        in_specs=placed,
        out_specs=(P("ep", "tp"), P("ep", "tp")),
        check_vma=False,
    )
```
